256 devices in a mesh: grp: 2 (over y), fs: 16 (over z), tp: 8 (over x, core).
Axes of the slice: x: 4, y: 2, z: 16, core: 2. Of those that a mesh axis runs over, the one named last changes fastest.
The devices are a block of a 4x16x16 slice.
Arguments:
- tokens: bfloat16 [32768, 2048], P(('grp', 'fs'), 'tp'), parts along dimension 0, may hold values from -50 to 50
- mix_gain: float32 [2048], replicated, may hold values from 0.1 to 1.9
- value_proj: bfloat16 [2048, 1024], P('fs', 'tp'), may hold values from -0.125 to 0.125
- gate_proj: bfloat16 [2048, 1024], P('fs', 'tp'), may hold values from -0.125 to 0.125
- conv_taps: float32 [31, 1024], P(None, 'tp'), may hold values from -1 to 1
- chan_gain: float32 [1024], replicated, may hold values from 0.1 to 1.9
- chan_shift: float32 [1024], replicated, may hold values from -3 to 3
- mix_out: bfloat16 [1024, 2048], P('fs', 'tp'), may hold values from -0.1875 to 0.1875
- mlp_gain: float32 [2048], replicated, may hold values from 0.1 to 1.9
- mlp_gate: bfloat16 [2048, 5632], P('fs', 'tp'), may hold values from -0.125 to 0.125
- mlp_up: bfloat16 [2048, 5632], P('fs', 'tp'), may hold values from -0.125 to 0.125
- gate_taps: float32 [3, 5632], P(None, 'tp'), may hold values from -3.5 to 3.5
- up_taps: float32 [3, 5632], P(None, 'tp'), may hold values from -3.5 to 3.5
- mlp_down: bfloat16 [5632, 2048], P('tp', 'fs'), may hold values from -0.078125 to 0.078125
- final_gain: float32 [2048], P('tp'), may hold values from 0.1 to 1.9
Outputs:
- layer_out: bfloat16 [32768, 2048], P(('grp', 'fs'), 'tp'), parts along dimension 0
The draws below stay inside these ranges and needn't reach their ends.
There are 2 independent parts, one for each index of `grp`. The reference program is written for one: setup_inputs(seed, part) draws one part's arguments, and reference() takes and returns one part's arrays. A program takes and returns all parts, laid end to end along the dimension named above; an argument that names none is the same for every part. Nothing has to cross between parts.
All inputs are finite; a program needn't handle non-finite values.
Results may differ from the reference program's by a relative error of at most 0.0095.
Values may be sent and summed in bfloat16 or wider, within the bound.
A program may use at most 128 MiB of HBM per device.

```python
import math
import jax
import jax.numpy as jnp
from jax import lax

D = 2048
CA = 1024
FF = 5632
KW = 31
FKW = 3
TOK_DEV = 1024
TOKENS = 16384
FF_BLOCK = 704
N_TP = 8


def draw_tokens(key, part):
    base_key = jax.random.fold_in(key, 7)
    key_rows, key_cols, key_vals = jax.random.split(base_key, 3)
    lowest = 0.3
    values = jnp.clip(jax.random.normal(key_vals, (TOKENS, D), jnp.float32), -4.0, 4.0)
    row_scale = jnp.exp(jax.random.uniform(key_rows, (TOKENS, 1), jnp.float32, math.log(lowest), math.log(3.0)))
    ramp = jnp.exp(jnp.linspace(math.log(0.4), math.log(2.5), D, dtype=jnp.float32))[None, :]
    col_scale = ramp * jnp.exp(jax.random.uniform(key_cols, (1, D), jnp.float32, -0.5, 0.5))
    return (values * row_scale * col_scale).astype(jnp.bfloat16)


def steps_of(key, dims, pieces, least, largest):
    level = 1.0
    for dim, blocks in pieces:
        draws = jax.random.uniform(jax.random.fold_in(jax.random.fold_in(key, 6), dim), (blocks,), jnp.float32, least / len(pieces), largest / len(pieces))
        level = level * jnp.repeat(jnp.exp(draws), dims[dim] // blocks).reshape((-1,) + (1,) * (len(dims) - 1 - dim))
    return level


def normal_values(own_key, extent, scale, reach, cuts=(), kind=jnp.bfloat16):
    array = scale * jax.random.normal(own_key, extent, jnp.float32)
    if cuts:
        array = array * steps_of(own_key, extent, cuts, -0.22, 0.18)
    return jnp.clip(array, -reach, reach).astype(kind)


def setup_inputs(seed: int = 0, part: int = 0) -> dict:
    splits = jax.random.split(jax.random.key(seed), 16)
    part_keys = jax.random.split(jax.random.fold_in(splits[15], part), 16)
    return {
        "tokens": draw_tokens(jax.random.fold_in(jax.random.fold_in(splits[15], part), 71), part),
        "mix_gain": jnp.clip(1.0 + 0.18 * jax.random.normal(splits[1], (D,), jnp.float32), 0.1, 1.9),
        "value_proj": normal_values(splits[2], (D, CA), D ** -0.5, 0.125, ((0, 16), (1, 8))),
        "gate_proj": normal_values(splits[3], (D, CA), D ** -0.5, 0.125, ((0, 16), (1, 8))),
        "conv_taps": normal_values(splits[4], (KW, CA), KW ** -0.5, 1.0, ((1, 8),), jnp.float32),
        "chan_gain": jnp.clip(1.0 + 0.18 * jax.random.normal(splits[5], (CA,), jnp.float32), 0.1, 1.9),
        "chan_shift": normal_values(splits[6], (CA,), 0.5, 3.0, (), jnp.float32),
        "mix_out": normal_values(splits[7], (CA, D), CA ** -0.5, 0.1875, ((0, 16), (1, 8))),
        "mlp_gain": jnp.clip(1.0 + 0.18 * jax.random.normal(splits[8], (D,), jnp.float32), 0.1, 1.9),
        "mlp_gate": normal_values(splits[9], (D, FF), D ** -0.5, 0.125, ((0, 16), (1, 8))),
        "mlp_up": normal_values(splits[10], (D, FF), D ** -0.5, 0.125, ((0, 16), (1, 8))),
        "gate_taps": normal_values(splits[11], (FKW, FF), FKW ** -0.5, 3.5, ((1, 8),), jnp.float32),
        "up_taps": normal_values(splits[12], (FKW, FF), FKW ** -0.5, 3.5, ((1, 8),), jnp.float32),
        "mlp_down": normal_values(splits[13], (FF, D), FF ** -0.5, 0.078125, ((0, 8), (1, 16))),
        "final_gain": jnp.clip(1.0 + 0.18 * jax.random.normal(splits[14], (D,), jnp.float32), 0.1, 1.9),
    }


def rms_scale(values, gain):
    return values * lax.rsqrt(lax.optimization_barrier(jnp.mean(values * values, axis=-1, keepdims=True)) + 1e-06) * gain

def along_sequences(values, taps, seq_len):
    width = taps.shape[0]
    half = (width - 1) // 2
    channels = values.shape[1]
    grouped = values.reshape(-1, seq_len, channels)
    padded = jnp.pad(grouped, ((0, 0), (half, width - 1 - half), (0, 0)))
    total = jnp.zeros_like(grouped)
    for offset in range(width):
        total = total + taps[offset] * padded[:, offset:offset + seq_len]
    return total.reshape(values.shape)

def reference(tokens, mix_gain, value_proj, gate_proj, conv_taps, chan_gain, chan_shift, mix_out, mlp_gain, mlp_gate, mlp_up, gate_taps, up_taps, mlp_down, final_gain):
    base = tokens.astype(jnp.float32)
    normed = rms_scale(base, mix_gain).astype(jnp.bfloat16)
    value = jnp.dot(normed, value_proj, preferred_element_type=jnp.float32)
    gate = jnp.dot(normed, gate_proj, preferred_element_type=jnp.float32)
    glu = value * jax.nn.sigmoid(gate)
    conv_out = along_sequences(glu, conv_taps, TOK_DEV).astype(jnp.bfloat16)
    conv_wide = conv_out.astype(jnp.float32)
    mean = lax.optimization_barrier(jnp.mean(conv_wide, axis=-1, keepdims=True))
    var = lax.optimization_barrier(jnp.mean(conv_wide * conv_wide, axis=-1, keepdims=True)) - mean * mean
    chan_norm = (conv_wide - mean) * lax.rsqrt(var + 1e-05) * chan_gain + chan_shift
    hidden_mix = jax.nn.silu(chan_norm).astype(jnp.bfloat16)
    mixed = (base + jnp.dot(hidden_mix, mix_out, preferred_element_type=jnp.float32)).astype(jnp.bfloat16)
    mixed_wide = mixed.astype(jnp.float32)
    normed_two = rms_scale(mixed_wide, mlp_gain).astype(jnp.bfloat16)
    gate_conv = along_sequences(jnp.dot(normed_two, mlp_gate, preferred_element_type=jnp.float32), gate_taps, TOK_DEV)
    up_conv = along_sequences(jnp.dot(normed_two, mlp_up, preferred_element_type=jnp.float32), up_taps, TOK_DEV)
    hidden_mlp = (jax.nn.silu(gate_conv) * up_conv).astype(jnp.bfloat16)
    mlp_out = jnp.zeros((tokens.shape[0], D), jnp.float32)
    for block in range(N_TP):
        lower = block * FF_BLOCK
        partial_sum = jnp.dot(hidden_mlp[:, lower:lower + FF_BLOCK], mlp_down[lower:lower + FF_BLOCK], preferred_element_type=jnp.float32)
        rounded = lax.optimization_barrier(partial_sum.astype(jnp.bfloat16))
        mlp_out = mlp_out + rounded.astype(jnp.float32)
    summed = mixed_wide + mlp_out
    return rms_scale(summed, final_gain).astype(jnp.bfloat16)
```

```python
import functools

import jax
import jax.numpy as jnp
from jax import lax
from jax.experimental import pallas as pl
from jax.experimental.pallas import tpu as pltpu
from jax.sharding import PartitionSpec as P

F32 = jnp.float32
BF16 = jnp.bfloat16
CHUNKS = 4
LANE = 128
PAD = 16
AB, CP, DP, CB0, CB1 = range(5)
TOK, CONV, MIX = range(3)


def body(
    sizes,
    tokens,
    mix_gain,
    value_own,
    gate_own,
    conv_taps,
    chan_gain,
    chan_shift,
    mix_out_own,
    mlp_gain,
    c_own,
    c_taps,
    d_own,
    final_gain,
    out,
    wab,
    wc,
    wd,
    tf,
    cf,
    mf,
    nrm,
    glu,
    gp,
    hm,
    hh,
    acc,
    qs,
    qr,
    fs_,
    fr,
    ns,
    nr,
    sm,
    ss_send,
    ss_recv,
    ob,
    lsem,
    zs,
    zr,
    ys,
    yr,
    xs,
    xr,
    rs,
    rr,
    ts,
    tr,
    osem,
):
    nf, nt = sizes
    nx = nt // 2
    half = nf // 2
    rows, fd = tokens.shape
    dm = tf.shape[1]
    ca = cf.shape[1]
    fc = ca // nt
    cr = rows // CHUNKS
    ffd = hh.shape[1]
    full_tiles = ffd // LANE * LANE
    tail = ffd - full_tiles
    kz = value_own.shape[0]
    kb = mix_out_own.shape[0]

    grp = lax.axis_index("grp")
    fs = lax.axis_index("fs")
    tp = lax.axis_index("tp")
    xi = tp // 2
    co = lax.rem(tp, 2)
    par = lax.rem(grp, 2)
    other = 1 - par

    def tp_of(dx, flip=False):
        core = 1 - co if flip else co
        return lax.rem(xi + dx + nx, nx) * 2 + core

    def dev_tp(t):
        return (grp, fs, t)

    def dev_fs(d):
        return (grp, lax.rem(fs + d + nf, nf), tp)

    peer_y = (grp + 1 - 2 * par, fs, tp)
    right, left, partner = dev_tp(tp_of(1)), dev_tp(tp_of(-1)), dev_tp(tp_of(0, True))
    zdev = (dev_fs(1), dev_fs(-1))

    def remote(src, dst, ssem, rsem, dev):
        return pltpu.make_async_remote_copy(
            src_ref=src,
            dst_ref=dst,
            send_sem=ssem,
            recv_sem=rsem,
            device_id=dev,
            device_id_type=pl.DeviceIdType.MESH,
        )

    sends = []

    def send(ref, ssem, rsem, dev, dst=None):
        copy = remote(ref, ref if dst is None else dst, ssem, rsem, dev)
        copy.start()
        sends.append(copy)

    def landed(ref, sem):
        remote(ref, ref, sem, sem, partner).wait_recv()

    def own_c(r0, n):
        return wc.at[fs, pl.ds(r0, n)]

    tok_cols = pl.ds(pl.multiple_of(tp * fd, fd), fd)
    moves = [
        (value_own, wab.at[fs, pl.ds(0, kz)]),
        (gate_own, wab.at[fs, pl.ds(kz, kz)]),
        (mix_out_own.at[:, pl.ds(0, LANE)], wab.at[fs, pl.ds(2 * kz, kb)]),
        (mix_out_own.at[:, pl.ds(LANE, LANE)], wab.at[fs, pl.ds(2 * kz + kb, kb)]),
        (tokens, tf.at[:, tok_cols]),
        (c_own, wc.at[fs]),
        (d_own, wd.at[fs]),
    ]
    local = [pltpu.make_async_copy(a, b, lsem.at[i]) for i, (a, b) in enumerate(moves)]
    for copy in local:
        copy.start()

    barrier = pltpu.get_barrier_semaphore()
    peers = [dev_tp(lax.rem(tp + o, nt)) for o in range(1, nt)] + [zdev[0], zdev[1], peer_y]
    for dev in peers:
        pl.semaphore_signal(barrier, inc=1, device_id=dev, device_id_type=pl.DeviceIdType.MESH)

    glu[pl.ds(0, PAD), :] = jnp.zeros((PAD, fc), F32)
    glu[pl.ds(PAD + rows, PAD), :] = jnp.zeros((PAD, fc), F32)
    gp[pl.ds(0, PAD), :] = jnp.zeros((PAD, gp.shape[1]), F32)
    gp[pl.ds(PAD + rows, PAD), :] = jnp.zeros((PAD, gp.shape[1]), F32)
    for copy in local:
        copy.wait()
    pl.semaphore_wait(barrier, len(peers))

    quarter = kz // 4
    dhalf = ffd // 2

    def zslice(lane, idx, h=None, who=None):
        who = par if who is None else who
        if lane == AB:
            ref, r0, n, step = wab, 0, wab.shape[1], 8
        elif lane == CP:
            ref, r0, n, step = wc, 2 * quarter + who * quarter, quarter, quarter
        elif lane == CB0:
            ref, r0, n, step = wc, 0, quarter, quarter
        elif lane == CB1:
            ref, r0, n, step = wc, quarter, quarter, quarter
        else:
            ref, r0, n, step = wd, who * dhalf, dhalf, dhalf
        if h is not None:
            r0, n = r0 + h * (n // 2), n // 2
        if not isinstance(r0, int):
            r0 = pl.multiple_of(r0, 16)
        return ref.at[idx, pl.ds(r0, n)]

    ylane = {CP: 0, DP: 1}

    def zidx(s, d):
        return lax.rem(fs - s + nf, nf) if d == 0 else lax.rem(fs + s, nf)

    def ymsg(s, d):
        return 2 * (s - 1) + d

    def z_own(lane):
        for d in range(2):
            send(zslice(lane, fs), zs.at[lane, 0, d], zr.at[lane, 1, d], zdev[d])

    def z_visit(lane, s):
        h = [None, None] if s < half else [0, 1]
        for d in range(2):
            idx = zidx(s, d)
            landed(zslice(lane, idx, h[d]), zr.at[lane, s, d])
            if s < half:
                piece = zslice(lane, idx, d if s == half - 1 else None)
                send(piece, zs.at[lane, s, d], zr.at[lane, s + 1, d], zdev[d])
        if lane in ylane:
            y = ylane[lane]
            for d in range(2):
                m = ymsg(s, d)
                send(zslice(lane, zidx(s, d), h[d]), ys.at[y, m], yr.at[y, m], peer_y)

    def y_done(lane):
        y = ylane[lane]
        for s in range(1, half + 1):
            for d in range(2):
                h = d if s == half else None
                landed(zslice(lane, zidx(s, d), h, other), yr.at[y, ymsg(s, d)])

    first, second = (AB, CP), (DP, CB0, CB1)
    visits = [(lane, s) for s in range(1, half + 1) for lane in first]
    visits += [(lane, s) for s in range(1, half + 1) for lane in second]
    queue = list(visits)

    def pump(n):
        for _ in range(min(n, len(queue))):
            lane, s = queue.pop(0)
            z_visit(lane, s)
            if (lane, s) == (first[-1], half - 1):
                for follow in second:
                    z_own(follow)

    def pump_to(lane, s):
        while (lane, s) in queue:
            pump(1)

    bufs = (tf, cf, mf)

    def blk(k, r, t, h=None):
        width = fc if k == CONV else fd
        r0, n = r * cr, cr
        if h is not None:
            r0, n = r0 + h * (cr // 2), cr // 2
        return bufs[k].at[pl.ds(r0, n), pl.ds(pl.multiple_of(t * width, width), width)]

    def ag_own(k, r):
        mine = blk(k, r, tp)
        send(mine, xs.at[k, r, 0], xr.at[k, r, 0], right)
        send(mine, xs.at[k, r, 1], xr.at[k, r, 1], left)
        send(mine, xs.at[k, r, 4], xr.at[k, r, 4], partner)

    def ag_v1(k, r):
        for d, (src, onward) in enumerate(((tp_of(-1), right), (tp_of(1), left))):
            landed(blk(k, r, src), xr.at[k, r, d])
            send(blk(k, r, src, d), xs.at[k, r, 2 + d], xr.at[k, r, 2 + d], onward)
            send(blk(k, r, src), xs.at[k, r, 5 + d], xr.at[k, r, 5 + d], partner)

    def ag_v2(k, r):
        for d in range(2):
            piece = blk(k, r, tp_of(2), d)
            landed(piece, xr.at[k, r, 2 + d])
            send(piece, xs.at[k, r, 7 + d], xr.at[k, r, 7 + d], partner)

    def ag_done(k, r):
        landed(blk(k, r, tp_of(0, True)), xr.at[k, r, 4])
        landed(blk(k, r, tp_of(-1, True)), xr.at[k, r, 5])
        landed(blk(k, r, tp_of(1, True)), xr.at[k, r, 6])
        landed(blk(k, r, tp_of(2, True), 0), xr.at[k, r, 7])
        landed(blk(k, r, tp_of(2, True), 1), xr.at[k, r, 8])

    tile = min(128, cr)

    def tiles(r, n, fn):
        def step(i, carry):
            fn(pl.multiple_of(r * cr + i * n, n))
            return carry

        lax.fori_loop(0, cr // n, step, 0)

    def norm(src, gain, r):
        def one(r0):
            total = jnp.zeros((tile, LANE), F32)
            for j in range(dm // LANE):
                v = src[pl.ds(r0, tile), pl.ds(j * LANE, LANE)].astype(F32)
                total = total + v * v
            scale = lax.rsqrt(jnp.sum(total, axis=-1, keepdims=True) / dm + 1e-06)
            for j in range(dm // LANE):
                cols = pl.ds(j * LANE, LANE)
                v = src[pl.ds(r0, tile), cols].astype(F32)
                nrm[pl.ds(r0, tile), cols] = (v * scale * gain[:, cols]).astype(BF16)

        tiles(r, tile, one)

    def mat_a(r):
        w = jnp.concatenate(
            [
                wab[:, 0:kz, :].reshape(dm, fc),
                wab[:, kz : 2 * kz, :].reshape(dm, fc),
            ],
            axis=1,
        )
        both = jnp.dot(nrm[pl.ds(r * cr, cr), :], w, preferred_element_type=F32)
        v, g = both[:, :fc], both[:, fc:]
        glu[pl.ds(PAD + r * cr, cr), :] = v / (1.0 + jnp.exp(-g))

    def conv(r):
        width = conv_taps.shape[0]
        base = PAD - (width - 1) // 2
        n = min(64, cr)

        def one(r0):
            total = jnp.zeros((n, fc), F32)
            for k in range(width):
                total = total + conv_taps[k : k + 1, :] * glu[pl.ds(r0 + base + k, n), :]
            cf[pl.ds(r0, n), pl.ds(pl.multiple_of(tp * fc, fc), fc)] = total.astype(BF16)

        tiles(r, n, one)

    def mix(r):
        def one(r0):
            s1 = jnp.zeros((tile, LANE), F32)
            s2 = jnp.zeros((tile, LANE), F32)
            for j in range(ca // LANE):
                v = cf[pl.ds(r0, tile), pl.ds(j * LANE, LANE)].astype(F32)
                s1 = s1 + v
                s2 = s2 + v * v
            mean = jnp.sum(s1, axis=-1, keepdims=True) / ca
            var = jnp.sum(s2, axis=-1, keepdims=True) / ca - mean * mean
            inv = lax.rsqrt(var + 1e-05)
            for j in range(ca // LANE):
                cols = pl.ds(j * LANE, LANE)
                v = cf[pl.ds(r0, tile), cols].astype(F32)
                v = (v - mean) * inv * chan_gain[:, cols] + chan_shift[:, cols]
                hm[pl.ds(r0, tile), cols] = (v / (1.0 + jnp.exp(-v))).astype(BF16)

        tiles(r, tile, one)
        w = jnp.concatenate(
            [
                wab[:, 2 * kz : 2 * kz + kb, :].reshape(ca, LANE),
                wab[:, 2 * kz + kb :, :].reshape(ca, LANE),
            ],
            axis=1,
        )
        here = pl.ds(r * cr, cr)
        prod = jnp.dot(hm[here, :], w, preferred_element_type=F32)
        mf[here, tok_cols] = (tf[here, tok_cols].astype(F32) + prod).astype(BF16)

    def mat_c(r):
        w = wc[...].reshape(dm, wc.shape[2])
        gp[pl.ds(PAD + r * cr, cr), :] = jnp.dot(
            nrm[pl.ds(r * cr, cr), :], w, preferred_element_type=F32
        )

    def hidden(r):
        n = min(64, cr)

        def conv3(r0, cols):
            window = gp[pl.ds(pl.multiple_of(r0 + PAD - 8, 8), n + 16), cols]
            total = c_taps[0:1, cols] * window[7 : 7 + n]
            for k in range(1, c_taps.shape[0]):
                total = total + c_taps[k : k + 1, cols] * window[7 + k : 7 + k + n]
            return total

        def one(r0):
            for j in range(full_tiles // LANE):
                g = conv3(r0, pl.ds(j * LANE, LANE))
                u = conv3(r0, pl.ds(full_tiles + j * LANE, LANE))
                hh[pl.ds(r0, n), pl.ds(j * LANE, LANE)] = (g / (1.0 + jnp.exp(-g)) * u).astype(BF16)
            v = conv3(r0, pl.ds(2 * full_tiles, LANE))
            u = pltpu.roll(v, LANE - tail, 1)
            h = (v / (1.0 + jnp.exp(-v)) * u).astype(BF16)
            hh[pl.ds(r0, n), pl.ds(full_tiles, tail)] = h[:, :tail]

        tiles(r, n, one)

    def down(r, m):
        w = jnp.concatenate([wd[2 * m], wd[2 * m + 1]], axis=1)
        return jnp.dot(hh[pl.ds(r * cr, cr), :], w, preferred_element_type=F32)

    hr = cr // 2

    def rs_a(r):
        for q in range(nx):
            qs[r, q] = down(r, 2 * q + 1 - co).astype(BF16)
        send(qs.at[r], rs.at[r, 0], rr.at[r, 0], partner, qr.at[r])
        for q in range(nx):
            acc[r, q] = down(r, 2 * q + co)

    xr1, xl1, xo = lax.rem(xi + 1, nx), lax.rem(xi + nx - 1, nx), lax.rem(xi + 2, nx)

    def rs_b(r):
        landed(qr.at[r], rr.at[r, 0])
        far = acc[r, xo] + qr[r, xo].astype(F32)
        fs_[r] = far.astype(BF16)
        send(fs_.at[r, pl.ds(0, hr)], rs.at[r, 1], rr.at[r, 1], right, fr.at[r, pl.ds(0, hr)])
        send(fs_.at[r, pl.ds(hr, hr)], rs.at[r, 2], rr.at[r, 2], left, fr.at[r, pl.ds(hr, hr)])

    def rs_c(r):
        for d, (q, onward) in enumerate(((xr1, right), (xl1, left))):
            landed(fr.at[r, pl.ds(d * hr, hr)], rr.at[r, 1 + d])
            gets, keeps = pl.ds(d * hr, hr), pl.ds((1 - d) * hr, hr)
            both = acc[r, q, gets] + qr[r, q, gets].astype(F32) + fr[r, gets].astype(F32)
            ns[r, d, gets] = both.astype(BF16)
            ns[r, d, keeps] = (acc[r, q, keeps] + qr[r, q, keeps].astype(F32)).astype(BF16)
            send(ns.at[r, d], rs.at[r, 3 + d], rr.at[r, 3 + d], onward, nr.at[r, d])

    def rs_d(r):
        here = pl.ds(r * cr, cr)
        total = acc[r, xi] + qr[r, xi].astype(F32) + mf[here, tok_cols].astype(F32)
        for d in range(2):
            landed(nr.at[r, d], rr.at[r, 3 + d])
        total = total + nr[r, 0].astype(F32) + nr[r, 1].astype(F32)
        sm[here, :] = total
        part = jnp.sum(total * total, axis=-1, keepdims=True)
        ss_send[r] = jnp.transpose(jnp.broadcast_to(part, (cr, LANE)))[0:8, :]
        for o in range(1, nt):
            send(
                ss_send.at[r],
                ts.at[r, o],
                tr.at[r, o],
                dev_tp(lax.rem(tp + o, nt)),
                ss_recv.at[r, o],
            )

    def rs_e(r):
        here = pl.ds(r * cr, cr)
        total = ss_send[r]
        for o in range(1, nt):
            landed(ss_recv.at[r, o], tr.at[r, o])
        for o in range(1, nt):
            total = total + ss_recv[r, o]
        wide = jnp.broadcast_to(total[0:1, :], (LANE, cr))
        scale = lax.rsqrt(jnp.transpose(wide)[:, 0:1] / dm + 1e-06)
        ob[here, :] = (sm[here, :] * scale * final_gain[...]).astype(BF16)
        pltpu.make_async_copy(ob.at[here, :], out.at[here, :], osem.at[r]).start()

    z_own(AB)
    z_own(CP)
    ag_own(TOK, 0)
    ag_own(TOK, 1)
    for r in range(CHUNKS):
        ag_v1(TOK, r)
        if r + 2 < CHUNKS:
            ag_own(TOK, r + 2)
        pump(1)
        if r >= 1:
            ag_v2(TOK, r - 1)
            ag_done(TOK, r - 1)
            norm(tf, mix_gain, r - 1)
        pump(1)
    ag_v2(TOK, CHUNKS - 1)
    ag_done(TOK, CHUNKS - 1)
    norm(tf, mix_gain, CHUNKS - 1)
    pump_to(AB, half)
    for r in range(CHUNKS):
        mat_a(r)
        if r >= 1:
            conv(r - 1)
            ag_own(CONV, r - 1)
        if r == 1:
            pump(1)
    conv(CHUNKS - 1)
    ag_own(CONV, CHUNKS - 1)
    pump(1)
    ag_v1(CONV, 0)
    ag_v1(CONV, 1)
    for r in range(CHUNKS):
        pump(1)
        ag_v2(CONV, r)
        if r + 2 < CHUNKS:
            ag_v1(CONV, r + 2)
        ag_done(CONV, r)
        mix(r)
        ag_own(MIX, r)
    pump(1)
    ag_v1(MIX, 0)
    pump(1)
    ag_v1(MIX, 1)
    for r in range(CHUNKS):
        pump(1)
        ag_v2(MIX, r)
        if r + 2 < CHUNKS:
            ag_v1(MIX, r + 2)
        pump(1)
        ag_done(MIX, r)
        norm(mf, mlp_gain, r)
    pump(len(queue))
    y_done(CP)
    last = CHUNKS - 1
    stages = (mat_c, None, hidden, rs_a, rs_b, rs_c, rs_d, rs_e)
    for tick in range(CHUNKS + len(stages) - 1):
        for lag in reversed(range(len(stages))):
            r = tick - lag
            if 0 <= r <= last and stages[lag] is not None:
                if lag == 3 and r == 0:
                    y_done(DP)
                stages[lag](r)

    for r in range(CHUNKS):
        here = pl.ds(r * cr, cr)
        pltpu.make_async_copy(ob.at[here, :], out.at[here, :], osem.at[r]).wait()
    for copy in sends:
        copy.wait_send()


def local(mesh, *args):
    (
        tokens,
        mix_gain,
        value_proj,
        gate_proj,
        conv_taps,
        chan_gain,
        chan_shift,
        mix_out,
        mlp_gain,
        mlp_gate,
        mlp_up,
        gate_taps,
        up_taps,
        mlp_down,
        final_gain,
    ) = args
    nf, nt = mesh.shape["fs"], mesh.shape["tp"]
    nx = nt // 2
    rows, fd = tokens.shape
    dm = mix_gain.shape[0]
    ca = chan_gain.shape[0]
    fc = value_proj.shape[1]
    kz, ffd = mlp_gate.shape
    kb = mix_out.shape[0]
    cr = rows // CHUNKS
    cut = ffd // LANE * LANE
    half = nf // 2

    def side(a, b):
        return jnp.concatenate([a[:, :cut], b[:, :cut], a[:, cut:], b[:, cut:]], axis=1)

    row = lambda v: v.reshape(1, -1)
    hbm = pl.BlockSpec(memory_space=pltpu.HBM)
    vmem = pl.BlockSpec(memory_space=pltpu.VMEM)
    dma = pltpu.SemaphoreType.DMA
    ny = 2 * half
    return pl.pallas_call(
        functools.partial(body, (nf, nt)),
        out_shape=jax.ShapeDtypeStruct((rows, fd), BF16),
        in_specs=[hbm, vmem, hbm, hbm, vmem, vmem, vmem, hbm, vmem, hbm, vmem, hbm, vmem],
        out_specs=hbm,
        scratch_shapes=[
            pltpu.VMEM((nf, 2 * kz + 2 * kb, LANE), BF16),
            pltpu.VMEM((nf, kz, 2 * ffd), BF16),
            pltpu.VMEM((nf, ffd, mlp_down.shape[1]), BF16),
            pltpu.VMEM((rows, dm), BF16),
            pltpu.VMEM((rows, ca), BF16),
            pltpu.VMEM((rows, dm), BF16),
            pltpu.VMEM((rows, dm), BF16),
            pltpu.VMEM((rows + 2 * PAD, fc), F32),
            pltpu.VMEM((rows + 2 * PAD, 2 * ffd), F32),
            pltpu.VMEM((rows, ca), BF16),
            pltpu.VMEM((rows, ffd), BF16),
            pltpu.VMEM((CHUNKS, nx, cr, fd), F32),
            pltpu.VMEM((CHUNKS, nx, cr, fd), BF16),
            pltpu.VMEM((CHUNKS, nx, cr, fd), BF16),
            pltpu.VMEM((CHUNKS, cr, fd), BF16),
            pltpu.VMEM((CHUNKS, cr, fd), BF16),
            pltpu.VMEM((CHUNKS, 2, cr, fd), BF16),
            pltpu.VMEM((CHUNKS, 2, cr, fd), BF16),
            pltpu.VMEM((rows, fd), F32),
            pltpu.VMEM((CHUNKS, 8, cr), F32),
            pltpu.VMEM((CHUNKS, nt, 8, cr), F32),
            pltpu.VMEM((rows, fd), BF16),
            dma((7,)),
            dma((5, half + 1, 2)),
            dma((5, half + 1, 2)),
            dma((2, ny)),
            dma((2, ny)),
            dma((3, CHUNKS, 9)),
            dma((3, CHUNKS, 9)),
            dma((CHUNKS, 5)),
            dma((CHUNKS, 5)),
            dma((CHUNKS, nt)),
            dma((CHUNKS, nt)),
            dma((CHUNKS,)),
        ],
        compiler_params=pltpu.CompilerParams(
            collective_id=0, has_side_effects=True, vmem_limit_bytes=67043328
        ),
        name="layer",
    )(
        tokens,
        row(mix_gain),
        value_proj,
        gate_proj,
        conv_taps,
        row(chan_gain),
        row(chan_shift),
        mix_out,
        row(mlp_gain),
        side(mlp_gate, mlp_up),
        side(gate_taps, up_taps),
        mlp_down,
        row(final_gain),
    )


def solution(mesh):
    return jax.shard_map(
        functools.partial(local, mesh),
        mesh=mesh,
        in_specs=(
            P(("grp", "fs"), "tp"),
            P(),
            P("fs", "tp"),
            P("fs", "tp"),
            P(None, "tp"),
            P(),
            P(),
            P("fs", "tp"),
            P(),
            P("fs", "tp"),
            P("fs", "tp"),
            P(None, "tp"),
            P(None, "tp"),
            P("tp", "fs"),
            P("tp"),
        ),
        out_specs=P(("grp", "fs"), "tp"),
        check_vma=False,
    )
```

```python
import functools

import jax
import jax.numpy as jnp
from jax import lax
from jax.experimental import pallas as pl
from jax.experimental.pallas import tpu as pltpu
from jax.sharding import PartitionSpec as P

F32 = jnp.float32
BF16 = jnp.bfloat16
CHUNKS = 4
RCHUNKS = 8
LANE = 128
PAD = 16
EACH = 3
VAL, GAT, OUT, CP0, CX, CP1, CA, CB, DA, DB = range(10)
TOK, CONV, MIX = range(3)


def body(
    sizes,
    tokens,
    mix_gain,
    value_own,
    gate_own,
    conv_taps,
    chan_gain,
    chan_shift,
    mix_out_own,
    mlp_gain,
    mlp_gate,
    mlp_up,
    gate_taps,
    up_taps,
    d_own,
    final_gain,
    out,
    wab,
    wc,
    wd,
    tf,
    cf,
    mf,
    nrm,
    glu,
    gp,
    hm,
    hh,
    acc,
    qs,
    qr,
    fs_,
    fr,
    ns,
    nr,
    sm,
    ss_send,
    ss_recv,
    gbuf,
    ubuf,
    c_taps,
    lsem,
    zs,
    zr,
    ys,
    yr,
    xs,
    xr,
    rs,
    rr,
    ts,
    tr,
):
    nf, nt = sizes
    nx = nt // 2
    half = nf // 2
    rows, fd = tokens.shape
    dm = tf.shape[1]
    ca = cf.shape[1]
    fc = ca // nt
    cr = rows // CHUNKS
    ffd = hh.shape[1]
    full_tiles = ffd // LANE * LANE
    tail = ffd - full_tiles
    kz = value_own.shape[0]
    kb = mix_out_own.shape[0]

    grp = lax.axis_index("grp")
    fs = lax.axis_index("fs")
    tp = lax.axis_index("tp")
    xi = tp // 2
    co = lax.rem(tp, 2)
    par = lax.rem(grp, 2)
    other = 1 - par

    def tp_of(dx, flip=False):
        core = 1 - co if flip else co
        return lax.rem(xi + dx + nx, nx) * 2 + core

    def dev_tp(t):
        return (grp, fs, t)

    def dev_fs(d):
        return (grp, lax.rem(fs + d + nf, nf), tp)

    peer_y = (grp + 1 - 2 * par, fs, tp)
    right, left, partner = dev_tp(tp_of(1)), dev_tp(tp_of(-1)), dev_tp(tp_of(0, True))
    zdev = (dev_fs(1), dev_fs(-1))

    def remote(src, dst, ssem, rsem, dev):
        return pltpu.make_async_remote_copy(
            src_ref=src,
            dst_ref=dst,
            send_sem=ssem,
            recv_sem=rsem,
            device_id=dev,
            device_id_type=pl.DeviceIdType.MESH,
        )

    def send(ref, ssem, rsem, dev, dst=None):
        remote(ref, ref if dst is None else dst, ssem, rsem, dev).start()

    def landed(ref, sem):
        remote(ref, ref, sem, sem, partner).wait_recv()

    def left_here(ref, sem):
        remote(ref, ref, sem, sem, partner).wait_send()

    def own_c(r0, n):
        return wc.at[fs, pl.ds(r0, n)]

    tok_cols = pl.ds(pl.multiple_of(tp * fd, fd), fd)
    moves = [
        (value_own, wab.at[fs, pl.ds(0, kz)]),
        (gate_own, wab.at[fs, pl.ds(kz, kz)]),
        (mix_out_own.at[:, pl.ds(0, LANE)], wab.at[fs, pl.ds(2 * kz, kb)]),
        (mix_out_own.at[:, pl.ds(LANE, LANE)], wab.at[fs, pl.ds(2 * kz + kb, kb)]),
        (tokens, tf.at[:, tok_cols]),
        (mlp_gate, gbuf),
        (mlp_up, ubuf),
        (d_own, wd.at[fs]),
    ]
    local = [pltpu.make_async_copy(a, b, lsem.at[i]) for i, (a, b) in enumerate(moves)]
    for copy in local:
        copy.start()

    barrier = pltpu.get_barrier_semaphore()
    peers = [dev_tp(lax.rem(tp + o, nt)) for o in range(1, nt)] + [zdev[0], zdev[1], peer_y]
    for dev in peers:
        pl.semaphore_signal(barrier, inc=1, device_id=dev, device_id_type=pl.DeviceIdType.MESH)

    whole = full_tiles // LANE
    cut = EACH * LANE
    at = 0
    for taps, lo, hi in (
        (gate_taps, 0, cut),
        (up_taps, 0, cut),
        (gate_taps, cut, full_tiles),
        (up_taps, cut, full_tiles),
        (gate_taps, full_tiles, ffd),
        (up_taps, full_tiles, ffd),
    ):
        c_taps[0 : taps.shape[0], at : at + hi - lo] = taps[:, lo:hi]
        at += hi - lo

    def pack(pos):
        if pos == 2 * whole:
            piece = jnp.concatenate([gbuf[full_tiles:, :], ubuf[full_tiles:, :]], axis=0)
        else:
            if pos < 2 * EACH:
                src, j = (gbuf, pos) if pos < EACH else (ubuf, pos - EACH)
            else:
                src, j = (gbuf, pos - EACH) if pos < EACH + whole else (ubuf, pos - whole)
            piece = src[j * LANE : (j + 1) * LANE, :]
        turned = jnp.transpose(piece.astype(F32)).astype(BF16)
        wc[fs, :, pos * LANE : (pos + 1) * LANE] = turned

    for i in (5, 6):
        local[i].wait()
    soon = (0, EACH, 2 * EACH)
    for pos in soon:
        pack(pos)

    glu[pl.ds(0, PAD), :] = jnp.zeros((PAD, fc), F32)
    glu[pl.ds(PAD + rows, PAD), :] = jnp.zeros((PAD, fc), F32)
    gp[pl.ds(0, PAD), :] = jnp.zeros((PAD, gp.shape[1]), F32)
    gp[pl.ds(PAD + rows, PAD), :] = jnp.zeros((PAD, gp.shape[1]), F32)
    for i, copy in enumerate(local):
        if i not in (5, 6):
            copy.wait()
    pl.semaphore_wait(barrier, len(peers))

    dhalf = ffd // 2
    lanes = {
        VAL: (wab, (0, kz), None),
        GAT: (wab, (kz, kz), None),
        OUT: (wab, (2 * kz, 2 * kb), None),
        CP0: (wc, None, (0, 1)),
        CX: (wc, None, (2 * EACH, 1)),
        CP1: (wc, None, (1, EACH - 1)),
        CA: (wc, None, (2 * EACH + 1, 2)),
        CB: (wc, None, (2 * EACH + 3, 2)),
        DA: (wd, (0, dhalf // 2), None),
        DB: (wd, (dhalf // 2, dhalf // 2), None),
    }
    ylane = {CP0: 0, CP1: 1, DA: 2, DB: 3}

    def zslice(lane, idx, h=None, who=None):
        who = par if who is None else who
        ref, span, cols = lanes[lane]
        r0, n = (0, ref.shape[1]) if span is None else span
        if lane in (DA, DB):
            r0 = pl.multiple_of(who * dhalf + r0, 16)
        if h is not None:
            r0, n = r0 + h * (n // 2), n // 2
        if not isinstance(r0, int):
            r0 = pl.multiple_of(r0, 8)
        if cols is None:
            return ref.at[idx, pl.ds(r0, n)]
        c0 = cols[0] * LANE
        if lane in (CP0, CP1):
            c0 = pl.multiple_of(who * (EACH * LANE) + c0, LANE)
        return ref.at[idx, pl.ds(r0, n), pl.ds(c0, cols[1] * LANE)]

    def zidx(s, d):
        return lax.rem(fs - s + nf, nf) if d == 0 else lax.rem(fs + s, nf)

    near = half // 2

    def z_own(lane):
        for d in range(2):
            send(zslice(lane, fs), zs.at[lane], zr.at[lane, 1, d], zdev[d])

    def z_visit(lane, s):
        h = [None, None] if s < half else [0, 1]
        for d in range(2):
            idx = zidx(s, d)
            landed(zslice(lane, idx, h[d]), zr.at[lane, s, d])
            if s < half:
                piece = zslice(lane, idx, d if s == half - 1 else None)
                send(piece, zs.at[lane], zr.at[lane, s + 1, d], zdev[d])
        if lane in ylane:
            y, part = ylane[lane], 0 if s <= near else 1
            for d in range(2):
                send(zslice(lane, zidx(s, d), h[d]), ys.at[y], yr.at[y, part], peer_y)

    def y_done(lane, part):
        count = 2 * near if part == 0 else nf - 1 - 2 * near
        landed(zslice(lane, pl.ds(0, count), None, other), yr.at[ylane[lane], part])

    phases = ((VAL, GAT, OUT, CP0, CX), (CP1, CA, CB, DA, DB))
    queue = [(lane, s) for group in phases for s in range(1, half + 1) for lane in group]

    def pump(n):
        for _ in range(min(n, len(queue))):
            lane, s = queue.pop(0)
            z_visit(lane, s)
            for now, later in zip(phases, phases[1:]):
                if s == half - 1 and lane == now[-1]:
                    for follow in later:
                        z_own(follow)

    def pump_to(lane, s):
        while (lane, s) in queue:
            pump(1)

    bufs = (tf, cf, mf)

    def blk(k, r, t, h=None):
        width = fc if k == CONV else fd
        r0, n = r * cr, cr
        if h is not None:
            r0, n = r0 + h * (cr // 2), cr // 2
        return bufs[k].at[pl.ds(r0, n), pl.ds(pl.multiple_of(t * width, width), width)]

    def ag_own(k, r):
        mine = blk(k, r, tp)
        send(mine, xs.at[k], xr.at[k, r, 0], right)
        send(mine, xs.at[k], xr.at[k, r, 1], left)
        send(mine, xs.at[k], xr.at[k, r, 4], partner)

    def ag_v1(k, r):
        for d, (src, onward) in enumerate(((tp_of(-1), right), (tp_of(1), left))):
            landed(blk(k, r, src), xr.at[k, r, d])
            send(blk(k, r, src, d), xs.at[k], xr.at[k, r, 2 + d], onward)
            send(blk(k, r, src), xs.at[k], xr.at[k, r, 4], partner)

    def ag_v2(k, r):
        for d in range(2):
            piece = blk(k, r, tp_of(2), d)
            landed(piece, xr.at[k, r, 2 + d])
            send(piece, xs.at[k], xr.at[k, r, 4], partner)

    def ag_done(k, r):
        width = fc if k == CONV else fd
        landed(bufs[k].at[pl.ds(r * cr, cr), pl.ds(0, nx * width)], xr.at[k, r, 4])

    tile = min(128, cr)

    def tiles(r, n, fn):
        def step(i, carry):
            fn(pl.multiple_of(r * cr + i * n, n))
            return carry

        lax.fori_loop(0, cr // n, step, 0)

    def norm(src, gain, r):
        def one(r0):
            total = jnp.zeros((tile, LANE), F32)
            for j in range(dm // LANE):
                v = src[pl.ds(r0, tile), pl.ds(j * LANE, LANE)].astype(F32)
                total = total + v * v
            scale = lax.rsqrt(jnp.sum(total, axis=-1, keepdims=True) / dm + 1e-06)
            for j in range(dm // LANE):
                cols = pl.ds(j * LANE, LANE)
                v = src[pl.ds(r0, tile), cols].astype(F32)
                nrm[pl.ds(r0, tile), cols] = (v * scale * gain[:, cols]).astype(BF16)

        tiles(r, tile, one)

    def mat_a(r):
        w = jnp.concatenate(
            [
                wab[:, 0:kz, :].reshape(dm, fc),
                wab[:, kz : 2 * kz, :].reshape(dm, fc),
            ],
            axis=1,
        )
        both = jnp.dot(nrm[pl.ds(r * cr, cr), :], w, preferred_element_type=F32)
        v, g = both[:, :fc], both[:, fc:]
        glu[pl.ds(PAD + r * cr, cr), :] = v / (1.0 + jnp.exp(-g))

    def conv(r):
        width = conv_taps.shape[0]
        base = PAD - (width - 1) // 2
        n = min(64, cr)

        def one(r0):
            total = jnp.zeros((n, fc), F32)
            for k in range(width):
                total = total + conv_taps[k : k + 1, :] * glu[pl.ds(r0 + base + k, n), :]
            cf[pl.ds(r0, n), pl.ds(pl.multiple_of(tp * fc, fc), fc)] = total.astype(BF16)

        tiles(r, n, one)

    def mix(r):
        def one(r0):
            s1 = jnp.zeros((tile, LANE), F32)
            s2 = jnp.zeros((tile, LANE), F32)
            for j in range(ca // LANE):
                v = cf[pl.ds(r0, tile), pl.ds(j * LANE, LANE)].astype(F32)
                s1 = s1 + v
                s2 = s2 + v * v
            mean = jnp.sum(s1, axis=-1, keepdims=True) / ca
            var = jnp.sum(s2, axis=-1, keepdims=True) / ca - mean * mean
            inv = lax.rsqrt(var + 1e-05)
            for j in range(ca // LANE):
                cols = pl.ds(j * LANE, LANE)
                v = cf[pl.ds(r0, tile), cols].astype(F32)
                v = (v - mean) * inv * chan_gain[:, cols] + chan_shift[:, cols]
                hm[pl.ds(r0, tile), cols] = (v / (1.0 + jnp.exp(-v))).astype(BF16)

        tiles(r, tile, one)
        w = jnp.concatenate(
            [
                wab[:, 2 * kz : 2 * kz + kb, :].reshape(ca, LANE),
                wab[:, 2 * kz + kb :, :].reshape(ca, LANE),
            ],
            axis=1,
        )
        here = pl.ds(r * cr, cr)
        prod = jnp.dot(hm[here, :], w, preferred_element_type=F32)
        mf[here, tok_cols] = (tf[here, tok_cols].astype(F32) + prod).astype(BF16)

    first_pairs = [(zidx(s, 0), zidx(s, 1)) for s in range(1, near + 1)]
    last_pairs = [(zidx(s, 0), zidx(s, 1)) for s in range(near + 1, half)] + [(fs, zidx(half, 0))]

    def pair_dots(r, pairs):
        here = pl.ds(r * cr, cr)
        total = None
        for pair in pairs:
            cols = [pl.ds(pl.multiple_of(i * kz, kz), kz) for i in pair]
            lhs = jnp.concatenate([nrm[here, c] for c in cols], axis=1)
            rhs = jnp.concatenate([wc[i] for i in pair], axis=0)
            term = jnp.dot(lhs, rhs, preferred_element_type=F32)
            total = term if total is None else total + term
        return total

    def mat_c(r):
        gp[pl.ds(PAD + r * cr, cr), :] = pair_dots(r, first_pairs)

    def mat_late(r):
        here = pl.ds(PAD + r * cr, cr)
        gp[here, :] = gp[here, :] + pair_dots(r, last_pairs)

    hr = rows // RCHUNKS
    hn = min(64, hr)

    def conv3(r0, at):
        cols = pl.ds(at * LANE, LANE)
        window = gp[pl.ds(pl.multiple_of(r0 + PAD - 8, 8), hn + 16), cols]
        total = c_taps[0:1, cols] * window[7 : 7 + hn]
        for k in range(1, gate_taps.shape[0]):
            total = total + c_taps[k : k + 1, cols] * window[7 + k : 7 + k + hn]
        return total

    def units(r0, j):
        g = conv3(r0, j if j < EACH else EACH + j)
        u = conv3(r0, EACH + j if j < EACH else whole + j)
        hh[pl.ds(r0, hn), pl.ds(j * LANE, LANE)] = (g / (1.0 + jnp.exp(-g)) * u).astype(BF16)

    def hidden(r):
        def step(i, carry):
            r0 = pl.multiple_of(r * hr + i * hn, hn)
            for j in range(whole):
                units(r0, j)
            v = conv3(r0, 2 * whole)
            u = pltpu.roll(v, LANE - tail, 1)
            h = (v / (1.0 + jnp.exp(-v)) * u).astype(BF16)
            hh[pl.ds(r0, hn), pl.ds(full_tiles, tail)] = h[:, :tail]
            return carry

        lax.fori_loop(0, hr // hn, step, 0)

    def down(r, m):
        w = jnp.concatenate([wd[2 * m], wd[2 * m + 1]], axis=1)
        return jnp.dot(hh[pl.ds(r * hr, hr), :], w, preferred_element_type=F32)

    hf = hr // 2

    def rs_a(r):
        for q in range(nx):
            qs[r, q] = down(r, 2 * q + 1 - co).astype(BF16)
        send(qs.at[r], rs.at[0], rr.at[r, 0], partner, qr.at[r])
        for q in range(nx):
            acc[r, q] = down(r, 2 * q + co)

    xr1, xl1, xo = lax.rem(xi + 1, nx), lax.rem(xi + nx - 1, nx), lax.rem(xi + 2, nx)

    def rs_b(r):
        landed(qr.at[r], rr.at[r, 0])
        far = acc[r, xo] + qr[r, xo].astype(F32)
        fs_[r] = far.astype(BF16)
        send(fs_.at[r, pl.ds(0, hf)], rs.at[1], rr.at[r, 1], right, fr.at[r, pl.ds(0, hf)])
        send(fs_.at[r, pl.ds(hf, hf)], rs.at[1], rr.at[r, 2], left, fr.at[r, pl.ds(hf, hf)])

    def rs_c(r):
        for d, (q, onward) in enumerate(((xr1, right), (xl1, left))):
            landed(fr.at[r, pl.ds(d * hf, hf)], rr.at[r, 1 + d])
            gets, keeps = pl.ds(d * hf, hf), pl.ds((1 - d) * hf, hf)
            both = acc[r, q, gets] + qr[r, q, gets].astype(F32) + fr[r, gets].astype(F32)
            ns[r, d, gets] = both.astype(BF16)
            ns[r, d, keeps] = (acc[r, q, keeps] + qr[r, q, keeps].astype(F32)).astype(BF16)
            send(ns.at[r, d], rs.at[2], rr.at[r, 3], onward, nr.at[r, d])

    def rs_d(r):
        here = pl.ds(r * hr, hr)
        total = acc[r, xi] + qr[r, xi].astype(F32) + mf[here, tok_cols].astype(F32)
        landed(nr.at[r], rr.at[r, 3])
        total = total + nr[r, 0].astype(F32) + nr[r, 1].astype(F32)
        sm[here, :] = total
        part = jnp.sum(total * total, axis=-1, keepdims=True)
        ss_send[r] = jnp.transpose(jnp.broadcast_to(part, (hr, LANE)))[0:8, :]
        for o in range(1, nt):
            send(
                ss_send.at[r],
                ts.at[0],
                tr.at[r],
                dev_tp(lax.rem(tp + o, nt)),
                ss_recv.at[r, o - 1],
            )

    def rs_e(r):
        here = pl.ds(r * hr, hr)
        total = ss_send[r]
        landed(ss_recv.at[r], tr.at[r])
        for o in range(nt - 1):
            total = total + ss_recv[r, o]
        wide = jnp.broadcast_to(total[0:1, :], (LANE, hr))
        scale = lax.rsqrt(jnp.transpose(wide)[:, 0:1] / dm + 1e-06)
        out[here, :] = (sm[here, :] * scale * final_gain[...]).astype(BF16)

    for lane in phases[0]:
        z_own(lane)
    ag_own(TOK, 0)
    ag_own(TOK, 1)
    for pos in range(2 * whole + 1):
        if pos not in soon:
            pack(pos)
    pump(5)
    ag_v1(TOK, 0)
    ag_own(TOK, 2)
    pump(5)
    ag_v1(TOK, 1)
    ag_own(TOK, 3)
    pump(5)
    ag_v2(TOK, 0)
    pump(3)
    ag_done(TOK, 0)
    norm(tf, mix_gain, 0)
    pump(2)
    ag_v1(TOK, 2)
    ag_v2(TOK, 1)
    pump(3)
    ag_done(TOK, 1)
    norm(tf, mix_gain, 1)
    pump(2)
    ag_v1(TOK, 3)
    pump(2)
    ag_v2(TOK, 2)
    pump(3)
    ag_done(TOK, 2)
    norm(tf, mix_gain, 2)
    ag_v2(TOK, 3)
    pump(3)
    ag_done(TOK, 3)
    norm(tf, mix_gain, 3)
    pump_to(GAT, half)
    mat_a(0)
    pump_to(CX, half)
    for r in range(1, CHUNKS):
        mat_a(r)
        conv(r - 1)
        ag_own(CONV, r - 1)
        pump(1)
    conv(CHUNKS - 1)
    ag_own(CONV, CHUNKS - 1)
    ag_v1(CONV, 0)
    pump(1)
    ag_v1(CONV, 1)
    pump(1)
    ag_v1(CONV, 2)
    pump(1)
    ag_v1(CONV, 3)
    pump(1)
    ag_v2(CONV, 0)
    ag_v2(CONV, 1)
    pump(1)
    for r in range(CHUNKS):
        ag_done(CONV, r)
        mix(r)
        ag_own(MIX, r)
        pump(1)
        if r + 2 < CHUNKS:
            ag_v2(CONV, r + 2)
    pump(1)
    for r in range(CHUNKS):
        pump(2)
        ag_v1(MIX, r)
    pump(1)
    for r in range(CHUNKS):
        ag_v2(MIX, r)
        pump(1)
    for r in range(CHUNKS):
        ag_done(MIX, r)
        norm(mf, mlp_gain, r)
        pump(1)
    pump_to(CB, near)
    y_done(CP0, 0)
    y_done(CP1, 0)
    for r in range(CHUNKS):
        mat_c(r)
        pump(2)
    pump(len(queue))
    y_done(CP0, 1)
    y_done(CP1, 1)
    stages = {2: hidden, 3: rs_a, 4: rs_b, 6: rs_c, 8: rs_d, 10: rs_e}
    per = cr // hr
    for tick in range(RCHUNKS + max(stages)):
        if tick % per == 0 and tick // per < CHUNKS:
            mat_late(tick // per)
        for lag in sorted(stages, reverse=True):
            r = tick - lag
            if 0 <= r < RCHUNKS:
                if lag == 3 and r == 0:
                    for lane in (DA, DB):
                        y_done(lane, 0)
                        y_done(lane, 1)
                stages[lag](r)

    for lane in lanes:
        left_here(zslice(lane, pl.ds(0, nf - 1)), zs.at[lane])
        if lane in ylane:
            left_here(zslice(lane, pl.ds(0, nf - 1)), ys.at[ylane[lane]])
    for k, width in ((TOK, fd), (CONV, fc), (MIX, fd)):
        left_here(bufs[k].at[:, pl.ds(0, (nt - 1) * width)], xs.at[k])
    for i, ref in enumerate((qs, fs_, ns)):
        left_here(ref, rs.at[i])
    left_here(ss_recv, ts.at[0])


def local(mesh, *args):
    (
        tokens,
        mix_gain,
        value_proj,
        gate_proj,
        conv_taps,
        chan_gain,
        chan_shift,
        mix_out,
        mlp_gain,
        mlp_gate,
        mlp_up,
        gate_taps,
        up_taps,
        mlp_down,
        final_gain,
    ) = args
    nf, nt = mesh.shape["fs"], mesh.shape["tp"]
    nx = nt // 2
    rows, fd = tokens.shape
    dm = mix_gain.shape[0]
    ca = chan_gain.shape[0]
    fc = value_proj.shape[1]
    kz, ffd = mlp_gate.shape
    kb = mix_out.shape[0]
    hr = rows // RCHUNKS
    half = nf // 2
    row = lambda v: v.reshape(1, -1)
    hbm = pl.BlockSpec(memory_space=pltpu.HBM)
    vmem = pl.BlockSpec(memory_space=pltpu.VMEM)
    dma = pltpu.SemaphoreType.DMA
    return pl.pallas_call(
        functools.partial(body, (nf, nt)),
        out_shape=jax.ShapeDtypeStruct((rows, fd), BF16),
        in_specs=[hbm, vmem, hbm, hbm, vmem, vmem, vmem, hbm, vmem, hbm, hbm, vmem, vmem, hbm, vmem],
        out_specs=vmem,
        scratch_shapes=[
            pltpu.VMEM((nf, 2 * kz + 2 * kb, LANE), BF16),
            pltpu.VMEM((nf, kz, 2 * ffd), BF16),
            pltpu.VMEM((nf, ffd, mlp_down.shape[1]), BF16),
            pltpu.VMEM((rows, dm), BF16),
            pltpu.VMEM((rows, ca), BF16),
            pltpu.VMEM((rows, dm), BF16),
            pltpu.VMEM((rows, dm), BF16),
            pltpu.VMEM((rows + 2 * PAD, fc), F32),
            pltpu.VMEM((rows + 2 * PAD, 2 * ffd), F32),
            pltpu.VMEM((rows, ca), BF16),
            pltpu.VMEM((rows, ffd), BF16),
            pltpu.VMEM((RCHUNKS, nx, hr, fd), F32),
            pltpu.VMEM((RCHUNKS, nx, hr, fd), BF16),
            pltpu.VMEM((RCHUNKS, nx, hr, fd), BF16),
            pltpu.VMEM((RCHUNKS, hr, fd), BF16),
            pltpu.VMEM((RCHUNKS, hr, fd), BF16),
            pltpu.VMEM((RCHUNKS, 2, hr, fd), BF16),
            pltpu.VMEM((RCHUNKS, 2, hr, fd), BF16),
            pltpu.VMEM((rows, fd), F32),
            pltpu.VMEM((RCHUNKS, 8, hr), F32),
            pltpu.VMEM((RCHUNKS, nt - 1, 8, hr), F32),
            pltpu.VMEM((ffd, kz), BF16),
            pltpu.VMEM((ffd, kz), BF16),
            pltpu.VMEM((8, 2 * ffd), F32),
            dma((8,)),
            dma((10,)),
            dma((10, half + 1, 2)),
            dma((4,)),
            dma((4, 2)),
            dma((3,)),
            dma((3, CHUNKS, 5)),
            dma((3,)),
            dma((RCHUNKS, 4)),
            dma((1,)),
            dma((RCHUNKS,)),
        ],
        compiler_params=pltpu.CompilerParams(
            collective_id=0, has_side_effects=True, vmem_limit_bytes=67043328
        ),
        name="layer",
    )(
        tokens,
        row(mix_gain),
        value_proj,
        gate_proj,
        conv_taps,
        row(chan_gain),
        row(chan_shift),
        mix_out,
        row(mlp_gain),
        mlp_gate.T,
        mlp_up.T,
        gate_taps,
        up_taps,
        mlp_down,
        row(final_gain),
    )


def solution(mesh):
    return jax.shard_map(
        functools.partial(local, mesh),
        mesh=mesh,
        in_specs=(
            P(("grp", "fs"), "tp"),
            P(),
            P("fs", "tp"),
            P("fs", "tp"),
            P(None, "tp"),
            P(),
            P(),
            P("fs", "tp"),
            P(),
            P("fs", "tp"),
            P("fs", "tp"),
            P(None, "tp"),
            P(None, "tp"),
            P("tp", "fs"),
            P("tp"),
        ),
        out_specs=P(("grp", "fs"), "tp"),
        check_vma=False,
    )
```

```python
import functools

import jax
import jax.numpy as jnp
from jax import lax
from jax.experimental import pallas as pl
from jax.experimental.pallas import tpu as pltpu
from jax.sharding import PartitionSpec as P

F32 = jnp.float32
BF16 = jnp.bfloat16
CHUNKS = 4
RCHUNKS = 8
LANE = 128
PAD = 16
EACH = 3
VAL, GAT, OUT, CP0, CP1, CP2, CA, CB, DN = range(9)
TOK, CONV, MIX = range(3)


def body(
    sizes,
    tokens,
    mix_gain,
    value_own,
    gate_own,
    conv_taps,
    chan_gain,
    chan_shift,
    mix_out_own,
    mlp_gain,
    mlp_gate,
    mlp_up,
    gate_taps,
    up_taps,
    d_own,
    final_gain,
    out,
    wab,
    wc,
    wd,
    tf,
    cf,
    mf,
    nrm,
    glu,
    gp,
    hm,
    hh,
    acc,
    qs,
    qr,
    fs_,
    fr,
    ns,
    nr,
    sm,
    ss_send,
    ss_recv,
    gbuf,
    ubuf,
    c_taps,
    lsem,
    zs,
    zr,
    ys,
    yr,
    xs,
    xr,
    rs,
    rr,
    ts,
    tr,
):
    nf, nt = sizes
    nx = nt // 2
    half = nf // 2
    rows, fd = tokens.shape
    dm = tf.shape[1]
    ca = cf.shape[1]
    fc = ca // nt
    cr = rows // CHUNKS
    ffd = hh.shape[1]
    full_tiles = ffd // LANE * LANE
    tail = ffd - full_tiles
    kz = value_own.shape[0]
    kb = mix_out_own.shape[0]

    grp = lax.axis_index("grp")
    fs = lax.axis_index("fs")
    tp = lax.axis_index("tp")
    xi = tp // 2
    co = lax.rem(tp, 2)
    par = lax.rem(grp, 2)
    other = 1 - par

    def tp_of(dx, flip=False):
        core = 1 - co if flip else co
        return lax.rem(xi + dx + nx, nx) * 2 + core

    def dev_tp(t):
        return (grp, fs, t)

    def dev_fs(d):
        return (grp, lax.rem(fs + d + nf, nf), tp)

    peer_y = (grp + 1 - 2 * par, fs, tp)
    right, left, partner = dev_tp(tp_of(1)), dev_tp(tp_of(-1)), dev_tp(tp_of(0, True))
    zdev = (dev_fs(1), dev_fs(-1))

    def remote(src, dst, ssem, rsem, dev):
        return pltpu.make_async_remote_copy(
            src_ref=src,
            dst_ref=dst,
            send_sem=ssem,
            recv_sem=rsem,
            device_id=dev,
            device_id_type=pl.DeviceIdType.MESH,
        )

    def send(ref, ssem, rsem, dev, dst=None):
        remote(ref, ref if dst is None else dst, ssem, rsem, dev).start()

    def landed(ref, sem):
        remote(ref, ref, sem, sem, partner).wait_recv()

    def left_here(ref, sem):
        remote(ref, ref, sem, sem, partner).wait_send()

    barrier = pltpu.get_barrier_semaphore()
    peers = [dev_tp(lax.rem(tp + o, nt)) for o in range(1, nt)] + [zdev[0], zdev[1], peer_y]
    for dev in peers:
        pl.semaphore_signal(barrier, inc=1, device_id=dev, device_id_type=pl.DeviceIdType.MESH)

    def own_c(r0, n):
        return wc.at[fs, pl.ds(r0, n)]

    tok_cols = pl.ds(pl.multiple_of(tp * fd, fd), fd)
    moves = [
        (value_own, wab.at[fs, pl.ds(0, kz)]),
        (gate_own, wab.at[fs, pl.ds(kz, kz)]),
        (mix_out_own.at[:, pl.ds(0, LANE)], wab.at[fs, pl.ds(2 * kz, kb)]),
        (mix_out_own.at[:, pl.ds(LANE, LANE)], wab.at[fs, pl.ds(2 * kz + kb, kb)]),
        (tokens, tf.at[:, tok_cols]),
        (mlp_gate, gbuf),
        (mlp_up, ubuf),
        (d_own, wd.at[fs]),
    ]
    local = [pltpu.make_async_copy(a, b, lsem.at[i]) for i, (a, b) in enumerate(moves)]
    for copy in local:
        copy.start()

    whole = full_tiles // LANE
    cut = EACH * LANE
    at = 0
    for taps, lo, hi in (
        (gate_taps, 0, cut),
        (up_taps, 0, cut),
        (gate_taps, cut, full_tiles),
        (up_taps, cut, full_tiles),
        (gate_taps, full_tiles, ffd),
        (up_taps, full_tiles, ffd),
    ):
        c_taps[0 : taps.shape[0], at : at + hi - lo] = taps[:, lo:hi]
        at += hi - lo

    def pack(pos):
        if pos == 2 * whole:
            piece = jnp.concatenate([gbuf[full_tiles:, :], ubuf[full_tiles:, :]], axis=0)
        else:
            if pos < 2 * EACH:
                src, j = (gbuf, pos) if pos < EACH else (ubuf, pos - EACH)
            else:
                src, j = (gbuf, pos - EACH) if pos < EACH + whole else (ubuf, pos - whole)
            piece = src[j * LANE : (j + 1) * LANE, :]
        turned = jnp.transpose(piece.astype(F32)).astype(BF16)
        wc[fs, :, pos * LANE : (pos + 1) * LANE] = turned

    for i in (5, 6):
        local[i].wait()
    soon = (0, 1, EACH, EACH + 1)
    for pos in soon:
        pack(pos)

    glu[pl.ds(0, PAD), :] = jnp.zeros((PAD, fc), F32)
    glu[pl.ds(PAD + rows, PAD), :] = jnp.zeros((PAD, fc), F32)
    gp[pl.ds(0, PAD), :] = jnp.zeros((PAD, gp.shape[1]), F32)
    gp[pl.ds(PAD + rows, PAD), :] = jnp.zeros((PAD, gp.shape[1]), F32)
    for i, copy in enumerate(local):
        if i not in (5, 6):
            copy.wait()
    pl.semaphore_wait(barrier, len(peers))

    dhalf = ffd // 2
    lanes = {
        VAL: (wab, (0, kz), None),
        GAT: (wab, (kz, kz), None),
        OUT: (wab, (2 * kz, 2 * kb), None),
        CP0: (wc, None, (0, 1)),
        CP1: (wc, None, (1, 1)),
        CP2: (wc, None, (2, EACH - 2)),
        CA: (wc, None, (2 * EACH, 2)),
        CB: (wc, None, (2 * EACH + 2, 3)),
        DN: (wd, (0, dhalf), None),
    }
    ylane = {CP0: 0, CP1: 1, CP2: 2, DN: 3}

    def zslice(lane, idx, h=None, who=None):
        who = par if who is None else who
        ref, span, cols = lanes[lane]
        r0, n = (0, ref.shape[1]) if span is None else span
        if lane == DN:
            r0 = pl.multiple_of(who * dhalf + r0, 16)
        if h is not None:
            r0, n = r0 + h * (n // 2), n // 2
        if not isinstance(r0, int):
            r0 = pl.multiple_of(r0, 8)
        if cols is None:
            return ref.at[idx, pl.ds(r0, n)]
        c0 = cols[0] * LANE
        if lane in (CP0, CP1, CP2):
            c0 = pl.multiple_of(who * (EACH * LANE) + c0, LANE)
        return ref.at[idx, pl.ds(r0, n), pl.ds(c0, cols[1] * LANE)]

    def zidx(s, d):
        return lax.rem(fs - s + nf, nf) if d == 0 else lax.rem(fs + s, nf)

    near = half // 2

    def z_own(lane):
        for d in range(2):
            send(zslice(lane, fs), zs.at[lane], zr.at[lane, 0, d], zdev[d])

    def z_visit(lane, s):
        h = [None, None] if s < half else [0, 1]
        for d in range(2):
            idx = zidx(s, d)
            landed(zslice(lane, idx, h[d]), zr.at[lane, s - 1, d])
            if s < half:
                piece = zslice(lane, idx, d if s == half - 1 else None)
                send(piece, zs.at[lane], zr.at[lane, s, d], zdev[d])
        if lane in ylane:
            y, part = ylane[lane], 0 if s <= near else 1
            for d in range(2):
                send(zslice(lane, zidx(s, d), h[d]), ys.at[y], yr.at[y, part], peer_y)

    def y_done(lane, part):
        count = 2 * near if part == 0 else nf - 1 - 2 * near
        landed(zslice(lane, pl.ds(0, count), None, other), yr.at[ylane[lane], part])

    phases = ((VAL, GAT, OUT, CP0, CP1), (CP2, DN, CA, CB))
    queue = [(lane, s) for group in phases for s in range(1, half + 1) for lane in group]

    def pump(n):
        for _ in range(min(n, len(queue))):
            lane, s = queue.pop(0)
            z_visit(lane, s)
            for now, later in zip(phases, phases[1:]):
                if s == half - 1 and lane == now[-1]:
                    for follow in later:
                        z_own(follow)

    def pump_to(lane, s):
        while (lane, s) in queue:
            pump(1)

    bufs = (tf, cf, mf)

    def blk(k, r, t, h=None):
        width = fc if k == CONV else fd
        r0, n = r * cr, cr
        if h is not None:
            r0, n = r0 + h * (cr // 2), cr // 2
        return bufs[k].at[pl.ds(r0, n), pl.ds(pl.multiple_of(t * width, width), width)]

    def ag_own(k, r):
        mine = blk(k, r, tp)
        send(mine, xs.at[k], xr.at[k, r, 0], right)
        send(mine, xs.at[k], xr.at[k, r, 1], left)
        send(mine, xs.at[k], xr.at[k, r, 4], partner)

    def ag_v1(k, r):
        for d, (src, onward) in enumerate(((tp_of(-1), right), (tp_of(1), left))):
            landed(blk(k, r, src), xr.at[k, r, d])
            send(blk(k, r, src, d), xs.at[k], xr.at[k, r, 2 + d], onward)
            send(blk(k, r, src), xs.at[k], xr.at[k, r, 4], partner)

    def ag_v2(k, r):
        for d in range(2):
            piece = blk(k, r, tp_of(2), d)
            landed(piece, xr.at[k, r, 2 + d])
            send(piece, xs.at[k], xr.at[k, r, 4], partner)

    def ag_done(k, r):
        width = fc if k == CONV else fd
        landed(bufs[k].at[pl.ds(r * cr, cr), pl.ds(0, nx * width)], xr.at[k, r, 4])

    tile = min(128, cr)

    def tiles(r, n, fn):
        def step(i, carry):
            fn(pl.multiple_of(r * cr + i * n, n))
            return carry

        lax.fori_loop(0, cr // n, step, 0)

    def norm(src, gain, r):
        def one(r0):
            total = jnp.zeros((tile, LANE), F32)
            for j in range(dm // LANE):
                v = src[pl.ds(r0, tile), pl.ds(j * LANE, LANE)].astype(F32)
                total = total + v * v
            scale = lax.rsqrt(jnp.sum(total, axis=-1, keepdims=True) / dm + 1e-06)
            for j in range(dm // LANE):
                cols = pl.ds(j * LANE, LANE)
                v = src[pl.ds(r0, tile), cols].astype(F32)
                nrm[pl.ds(r0, tile), cols] = (v * scale * gain[:, cols]).astype(BF16)

        tiles(r, tile, one)

    def mat_a(r):
        w = jnp.concatenate(
            [
                wab[:, 0:kz, :].reshape(dm, fc),
                wab[:, kz : 2 * kz, :].reshape(dm, fc),
            ],
            axis=1,
        )
        both = jnp.dot(nrm[pl.ds(r * cr, cr), :], w, preferred_element_type=F32)
        v, g = both[:, :fc], both[:, fc:]
        glu[pl.ds(PAD + r * cr, cr), :] = v / (1.0 + jnp.exp(-g))

    def conv(r):
        width = conv_taps.shape[0]
        base = PAD - (width - 1) // 2
        n = min(64, cr)

        def one(r0):
            total = jnp.zeros((n, fc), F32)
            for k in range(width):
                total = total + conv_taps[k : k + 1, :] * glu[pl.ds(r0 + base + k, n), :]
            cf[pl.ds(r0, n), pl.ds(pl.multiple_of(tp * fc, fc), fc)] = total.astype(BF16)

        tiles(r, n, one)

    def mix(r):
        def one(r0):
            s1 = jnp.zeros((tile, LANE), F32)
            s2 = jnp.zeros((tile, LANE), F32)
            for j in range(ca // LANE):
                v = cf[pl.ds(r0, tile), pl.ds(j * LANE, LANE)].astype(F32)
                s1 = s1 + v
                s2 = s2 + v * v
            mean = jnp.sum(s1, axis=-1, keepdims=True) / ca
            var = jnp.sum(s2, axis=-1, keepdims=True) / ca - mean * mean
            inv = lax.rsqrt(var + 1e-05)
            for j in range(ca // LANE):
                cols = pl.ds(j * LANE, LANE)
                v = cf[pl.ds(r0, tile), cols].astype(F32)
                v = (v - mean) * inv * chan_gain[:, cols] + chan_shift[:, cols]
                hm[pl.ds(r0, tile), cols] = (v / (1.0 + jnp.exp(-v))).astype(BF16)

        tiles(r, tile, one)
        w = jnp.concatenate(
            [
                wab[:, 2 * kz : 2 * kz + kb, :].reshape(ca, LANE),
                wab[:, 2 * kz + kb :, :].reshape(ca, LANE),
            ],
            axis=1,
        )
        here = pl.ds(r * cr, cr)
        prod = jnp.dot(hm[here, :], w, preferred_element_type=F32)
        mf[here, tok_cols] = (tf[here, tok_cols].astype(F32) + prod).astype(BF16)

    first_pairs = [(zidx(s, 0), zidx(s, 1)) for s in range(1, near + 1)]
    last_pairs = [(zidx(s, 0), zidx(s, 1)) for s in range(near + 1, half)] + [(fs, zidx(half, 0))]

    def pair_dots(r, pairs):
        here = pl.ds(r * cr, cr)
        total = None
        for pair in pairs:
            cols = [pl.ds(pl.multiple_of(i * kz, kz), kz) for i in pair]
            lhs = jnp.concatenate([nrm[here, c] for c in cols], axis=1)
            rhs = jnp.concatenate([wc[i] for i in pair], axis=0)
            term = jnp.dot(lhs, rhs, preferred_element_type=F32)
            total = term if total is None else total + term
        return total

    def mat_c(r):
        gp[pl.ds(PAD + r * cr, cr), :] = pair_dots(r, first_pairs)

    def mat_late(r):
        here = pl.ds(PAD + r * cr, cr)
        gp[here, :] = gp[here, :] + pair_dots(r, last_pairs)

    hr = rows // RCHUNKS
    hn = min(64, hr)

    def conv3(r0, at):
        cols = pl.ds(at * LANE, LANE)
        window = gp[pl.ds(pl.multiple_of(r0 + PAD - 8, 8), hn + 16), cols]
        total = c_taps[0:1, cols] * window[7 : 7 + hn]
        for k in range(1, gate_taps.shape[0]):
            total = total + c_taps[k : k + 1, cols] * window[7 + k : 7 + k + hn]
        return total

    def units(r0, j):
        g = conv3(r0, j if j < EACH else EACH + j)
        u = conv3(r0, EACH + j if j < EACH else whole + j)
        hh[pl.ds(r0, hn), pl.ds(j * LANE, LANE)] = (g / (1.0 + jnp.exp(-g)) * u).astype(BF16)

    def hidden(r):
        def step(i, carry):
            r0 = pl.multiple_of(r * hr + i * hn, hn)
            for j in range(whole):
                units(r0, j)
            v = conv3(r0, 2 * whole)
            u = pltpu.roll(v, LANE - tail, 1)
            h = (v / (1.0 + jnp.exp(-v)) * u).astype(BF16)
            hh[pl.ds(r0, hn), pl.ds(full_tiles, tail)] = h[:, :tail]
            return carry

        lax.fori_loop(0, hr // hn, step, 0)

    def down(r, m):
        w = jnp.concatenate([wd[2 * m], wd[2 * m + 1]], axis=1)
        return jnp.dot(hh[pl.ds(r * hr, hr), :], w, preferred_element_type=F32)

    hf = hr // 2

    def rs_a(r):
        for q in range(nx):
            qs[r, q] = down(r, 2 * q + 1 - co).astype(BF16)
        send(qs.at[r], rs.at[0], rr.at[r, 0], partner, qr.at[r])
        for q in range(nx):
            acc[r, q] = down(r, 2 * q + co)

    xr1, xl1, xo = lax.rem(xi + 1, nx), lax.rem(xi + nx - 1, nx), lax.rem(xi + 2, nx)

    def rs_b(r):
        landed(qr.at[r], rr.at[r, 0])
        far = acc[r, xo] + qr[r, xo].astype(F32)
        fs_[r] = far.astype(BF16)
        send(fs_.at[r, pl.ds(0, hf)], rs.at[1], rr.at[r, 1], right, fr.at[r, pl.ds(0, hf)])
        send(fs_.at[r, pl.ds(hf, hf)], rs.at[1], rr.at[r, 2], left, fr.at[r, pl.ds(hf, hf)])

    def rs_c(r):
        for d, (q, onward) in enumerate(((xr1, right), (xl1, left))):
            landed(fr.at[r, pl.ds(d * hf, hf)], rr.at[r, 1 + d])
            gets, keeps = pl.ds(d * hf, hf), pl.ds((1 - d) * hf, hf)
            both = acc[r, q, gets] + qr[r, q, gets].astype(F32) + fr[r, gets].astype(F32)
            ns[r, d, gets] = both.astype(BF16)
            ns[r, d, keeps] = (acc[r, q, keeps] + qr[r, q, keeps].astype(F32)).astype(BF16)
            send(ns.at[r, d], rs.at[2], rr.at[r, 3], onward, nr.at[r, d])

    def rs_d(r):
        here = pl.ds(r * hr, hr)
        total = acc[r, xi] + qr[r, xi].astype(F32) + mf[here, tok_cols].astype(F32)
        landed(nr.at[r], rr.at[r, 3])
        total = total + nr[r, 0].astype(F32) + nr[r, 1].astype(F32)
        sm[here, :] = total
        part = jnp.sum(total * total, axis=-1, keepdims=True)
        ss_send[r] = jnp.transpose(jnp.broadcast_to(part, (hr, LANE)))[0:8, :]
        for o in range(1, nt):
            send(
                ss_send.at[r],
                ts.at[0],
                tr.at[r],
                dev_tp(lax.rem(tp + o, nt)),
                ss_recv.at[r, o - 1],
            )

    def rs_e(r):
        here = pl.ds(r * hr, hr)
        total = ss_send[r]
        landed(ss_recv.at[r], tr.at[r])
        for o in range(nt - 1):
            total = total + ss_recv[r, o]
        wide = jnp.broadcast_to(total[0:1, :], (LANE, hr))
        scale = lax.rsqrt(jnp.transpose(wide)[:, 0:1] / dm + 1e-06)
        out[here, :] = (sm[here, :] * scale * final_gain[...]).astype(BF16)

    for lane in phases[0]:
        z_own(lane)
    ag_own(TOK, 0)
    ag_own(TOK, 1)
    for pos in range(2 * whole + 1):
        if pos not in soon:
            pack(pos)
    pump(5)
    ag_v1(TOK, 0)
    ag_own(TOK, 2)
    pump(5)
    ag_v1(TOK, 1)
    ag_own(TOK, 3)
    pump(5)
    ag_v2(TOK, 0)
    pump(3)
    ag_done(TOK, 0)
    norm(tf, mix_gain, 0)
    pump(2)
    ag_v1(TOK, 2)
    ag_v2(TOK, 1)
    pump(3)
    ag_done(TOK, 1)
    norm(tf, mix_gain, 1)
    pump(2)
    ag_v1(TOK, 3)
    pump(2)
    ag_v2(TOK, 2)
    pump(3)
    ag_done(TOK, 2)
    norm(tf, mix_gain, 2)
    ag_v2(TOK, 3)
    pump(3)
    ag_done(TOK, 3)
    norm(tf, mix_gain, 3)
    pump_to(GAT, half)
    mat_a(0)
    pump_to(CP1, half)
    for r in range(1, CHUNKS):
        mat_a(r)
        conv(r - 1)
        ag_own(CONV, r - 1)
        pump(1)
    conv(CHUNKS - 1)
    ag_own(CONV, CHUNKS - 1)
    ag_v1(CONV, 0)
    pump(1)
    ag_v1(CONV, 1)
    ag_v1(CONV, 2)
    pump(1)
    ag_v1(CONV, 3)
    pump(1)
    ag_v2(CONV, 0)
    ag_v2(CONV, 1)
    pump(1)
    for r in range(CHUNKS):
        ag_done(CONV, r)
        mix(r)
        ag_own(MIX, r)
        if r != 1:
            pump(1)
        if r + 2 < CHUNKS:
            ag_v2(CONV, r + 2)
    pump(1)
    for r in range(CHUNKS):
        pump(2)
        ag_v1(MIX, r)
    pump(1)
    for r in range(CHUNKS):
        ag_v2(MIX, r)
        pump(1)
    for r in range(CHUNKS):
        ag_done(MIX, r)
        norm(mf, mlp_gain, r)
        pump(1)
    pump_to(CB, near)
    for lane in (CP0, CP1, CP2):
        y_done(lane, 0)
    for r in range(CHUNKS):
        mat_c(r)
        pump(2)
    pump(len(queue))
    for lane in (CP0, CP1, CP2):
        y_done(lane, 1)
    stages = {1: rs_b, 3: rs_c, 7: rs_d, 10: rs_e}
    per = cr // hr
    for tick in range(RCHUNKS + max(stages)):
        for lag, stage in stages.items():
            if 0 <= tick - lag < RCHUNKS:
                stage(tick - lag)
        if tick < RCHUNKS:
            if tick == 0:
                mat_late(0)
            if tick % per == per - 1 and tick // per + 1 < CHUNKS:
                mat_late(tick // per + 1)
            hidden(tick)
            if tick == 0:
                y_done(DN, 0)
                y_done(DN, 1)
            rs_a(tick)

    for lane in lanes:
        left_here(zslice(lane, pl.ds(0, nf - 1)), zs.at[lane])
        if lane in ylane:
            left_here(zslice(lane, pl.ds(0, nf - 1)), ys.at[ylane[lane]])
    for k, width in ((TOK, fd), (CONV, fc), (MIX, fd)):
        left_here(bufs[k].at[:, pl.ds(0, (nt - 1) * width)], xs.at[k])
    for i, ref in enumerate((qs, fs_, ns)):
        left_here(ref, rs.at[i])
    left_here(ss_recv, ts.at[0])


def local(mesh, *args):
    (
        tokens,
        mix_gain,
        value_proj,
        gate_proj,
        conv_taps,
        chan_gain,
        chan_shift,
        mix_out,
        mlp_gain,
        mlp_gate,
        mlp_up,
        gate_taps,
        up_taps,
        mlp_down,
        final_gain,
    ) = args
    nf, nt = mesh.shape["fs"], mesh.shape["tp"]
    nx = nt // 2
    rows, fd = tokens.shape
    dm = mix_gain.shape[0]
    ca = chan_gain.shape[0]
    fc = value_proj.shape[1]
    kz, ffd = mlp_gate.shape
    kb = mix_out.shape[0]
    hr = rows // RCHUNKS
    half = nf // 2
    row = lambda v: v.reshape(1, -1)
    hbm = pl.BlockSpec(memory_space=pltpu.HBM)
    vmem = pl.BlockSpec(memory_space=pltpu.VMEM)
    dma = pltpu.SemaphoreType.DMA
    return pl.pallas_call(
        functools.partial(body, (nf, nt)),
        out_shape=jax.ShapeDtypeStruct((rows, fd), BF16),
        in_specs=[hbm, vmem, hbm, hbm, vmem, vmem, vmem, hbm, vmem, hbm, hbm, vmem, vmem, hbm, vmem],
        out_specs=vmem,
        scratch_shapes=[
            pltpu.VMEM((nf, 2 * kz + 2 * kb, LANE), BF16),
            pltpu.VMEM((nf, kz, 2 * ffd), BF16),
            pltpu.VMEM((nf, ffd, mlp_down.shape[1]), BF16),
            pltpu.VMEM((rows, dm), BF16),
            pltpu.VMEM((rows, ca), BF16),
            pltpu.VMEM((rows, dm), BF16),
            pltpu.VMEM((rows, dm), BF16),
            pltpu.VMEM((rows + 2 * PAD, fc), F32),
            pltpu.VMEM((rows + 2 * PAD, 2 * ffd), F32),
            pltpu.VMEM((rows, ca), BF16),
            pltpu.VMEM((rows, ffd), BF16),
            pltpu.VMEM((RCHUNKS, nx, hr, fd), F32),
            pltpu.VMEM((RCHUNKS, nx, hr, fd), BF16),
            pltpu.VMEM((RCHUNKS, nx, hr, fd), BF16),
            pltpu.VMEM((RCHUNKS, hr, fd), BF16),
            pltpu.VMEM((RCHUNKS, hr, fd), BF16),
            pltpu.VMEM((RCHUNKS, 2, hr, fd), BF16),
            pltpu.VMEM((RCHUNKS, 2, hr, fd), BF16),
            pltpu.VMEM((rows, fd), F32),
            pltpu.VMEM((RCHUNKS, 8, hr), F32),
            pltpu.VMEM((RCHUNKS, nt - 1, 8, hr), F32),
            pltpu.VMEM((ffd, kz), BF16),
            pltpu.VMEM((ffd, kz), BF16),
            pltpu.VMEM((8, 2 * ffd), F32),
            dma((8,)),
            dma((9,)),
            dma((9, half, 2)),
            dma((4,)),
            dma((4, 2)),
            dma((3,)),
            dma((3, CHUNKS, 5)),
            dma((3,)),
            dma((RCHUNKS, 4)),
            dma((1,)),
            dma((RCHUNKS,)),
        ],
        compiler_params=pltpu.CompilerParams(
            collective_id=0, has_side_effects=True, vmem_limit_bytes=67043328
        ),
        name="layer",
    )(
        tokens,
        row(mix_gain),
        value_proj,
        gate_proj,
        conv_taps,
        row(chan_gain),
        row(chan_shift),
        mix_out,
        row(mlp_gain),
        mlp_gate.T,
        mlp_up.T,
        gate_taps,
        up_taps,
        mlp_down,
        row(final_gain),
    )


def solution(mesh):
    return jax.shard_map(
        functools.partial(local, mesh),
        mesh=mesh,
        in_specs=(
            P(("grp", "fs"), "tp"),
            P(),
            P("fs", "tp"),
            P("fs", "tp"),
            P(None, "tp"),
            P(),
            P(),
            P("fs", "tp"),
            P(),
            P("fs", "tp"),
            P("fs", "tp"),
            P(None, "tp"),
            P(None, "tp"),
            P("tp", "fs"),
            P("tp"),
        ),
        out_specs=P(("grp", "fs"), "tp"),
        check_vma=False,
    )
```

```python
import functools

import jax
import jax.numpy as jnp
from jax import lax
from jax.experimental import pallas as pl
from jax.experimental.pallas import tpu as pltpu
from jax.sharding import PartitionSpec as P

F32 = jnp.float32
BF16 = jnp.bfloat16
CHUNKS = 4
RCHUNKS = 8
LANE = 128
PAD = 16
EACH = 3
VAL, GAT, OUT, CP0, CP1, CP2, CS, CA, CB, DN = range(10)
TOK, CONV, MIX = range(3)


def body(
    sizes,
    tokens,
    mix_gain,
    value_own,
    gate_own,
    conv_taps,
    chan_gain,
    chan_shift,
    mix_out_own,
    mlp_gain,
    mlp_gate,
    mlp_up,
    gate_taps,
    up_taps,
    d_own,
    final_gain,
    out,
    wab,
    wc,
    wd,
    tf,
    cf,
    mf,
    nrm,
    glu,
    gp,
    hm,
    hh,
    acc,
    qs,
    qr,
    fs_,
    fr,
    ns,
    nr,
    sm,
    ss_send,
    ss_recv,
    gbuf,
    ubuf,
    c_taps,
    lsem,
    zs,
    zr,
    ys,
    yr,
    xs,
    xr,
    rs,
    rr,
    ts,
    tr,
):
    nf, nt = sizes
    nx = nt // 2
    half = nf // 2
    rows, fd = tokens.shape
    dm = tf.shape[1]
    ca = cf.shape[1]
    fc = ca // nt
    cr = rows // CHUNKS
    ffd = hh.shape[1]
    full_tiles = ffd // LANE * LANE
    tail = ffd - full_tiles
    kz = value_own.shape[0]
    kb = mix_out_own.shape[0]

    grp = lax.axis_index("grp")
    fs = lax.axis_index("fs")
    tp = lax.axis_index("tp")
    xi = tp // 2
    co = lax.rem(tp, 2)
    par = lax.rem(grp, 2)
    other = 1 - par

    def tp_of(dx, flip=False):
        core = 1 - co if flip else co
        return lax.rem(xi + dx + nx, nx) * 2 + core

    def dev_tp(t):
        return (grp, fs, t)

    def dev_fs(d):
        return (grp, lax.rem(fs + d + nf, nf), tp)

    peer_y = (grp + 1 - 2 * par, fs, tp)
    right, left, partner = dev_tp(tp_of(1)), dev_tp(tp_of(-1)), dev_tp(tp_of(0, True))
    zdev = (dev_fs(1), dev_fs(-1))

    def remote(src, dst, ssem, rsem, dev):
        return pltpu.make_async_remote_copy(
            src_ref=src,
            dst_ref=dst,
            send_sem=ssem,
            recv_sem=rsem,
            device_id=dev,
            device_id_type=pl.DeviceIdType.MESH,
        )

    def send(ref, ssem, rsem, dev, dst=None):
        remote(ref, ref if dst is None else dst, ssem, rsem, dev).start()

    def landed(ref, sem):
        remote(ref, ref, sem, sem, partner).wait_recv()

    def left_here(ref, sem):
        remote(ref, ref, sem, sem, partner).wait_send()

    barrier = pltpu.get_barrier_semaphore()
    peers = [dev_tp(lax.rem(tp + o, nt)) for o in range(1, nt)] + [zdev[0], zdev[1], peer_y]
    for dev in peers:
        pl.semaphore_signal(barrier, inc=1, device_id=dev, device_id_type=pl.DeviceIdType.MESH)

    def own_c(r0, n):
        return wc.at[fs, pl.ds(r0, n)]

    tok_cols = pl.ds(pl.multiple_of(tp * fd, fd), fd)
    moves = [
        (value_own, wab.at[fs, pl.ds(0, kz)]),
        (gate_own, wab.at[fs, pl.ds(kz, kz)]),
        (mix_out_own.at[:, pl.ds(0, LANE)], wab.at[fs, pl.ds(2 * kz, kb)]),
        (mix_out_own.at[:, pl.ds(LANE, LANE)], wab.at[fs, pl.ds(2 * kz + kb, kb)]),
        (tokens, tf.at[:, tok_cols]),
        (mlp_gate, gbuf),
        (mlp_up, ubuf),
        (d_own, wd.at[fs]),
    ]
    local = [pltpu.make_async_copy(a, b, lsem.at[i]) for i, (a, b) in enumerate(moves)]
    for copy in local:
        copy.start()

    whole = full_tiles // LANE
    cut = EACH * LANE
    at = 0
    for taps, lo, hi in (
        (gate_taps, 0, cut),
        (up_taps, 0, cut),
        (gate_taps, cut, full_tiles),
        (up_taps, cut, full_tiles),
        (gate_taps, full_tiles, ffd),
        (up_taps, full_tiles, ffd),
    ):
        c_taps[0 : taps.shape[0], at : at + hi - lo] = taps[:, lo:hi]
        at += hi - lo

    def pack(pos):
        if pos == 2 * whole:
            piece = jnp.concatenate([gbuf[full_tiles:, :], ubuf[full_tiles:, :]], axis=0)
        else:
            if pos < 2 * EACH:
                src, j = (gbuf, pos) if pos < EACH else (ubuf, pos - EACH)
            else:
                src, j = (gbuf, pos - EACH) if pos < EACH + whole else (ubuf, pos - whole)
            piece = src[j * LANE : (j + 1) * LANE, :]
        turned = jnp.transpose(piece.astype(F32)).astype(BF16)
        wc[fs, :, pos * LANE : (pos + 1) * LANE] = turned

    for i in (5, 6):
        local[i].wait()
    soon = (0, 1, EACH, EACH + 1)
    for pos in soon:
        pack(pos)

    glu[pl.ds(0, PAD), :] = jnp.zeros((PAD, fc), F32)
    glu[pl.ds(PAD + rows, PAD), :] = jnp.zeros((PAD, fc), F32)
    gp[pl.ds(0, PAD), :] = jnp.zeros((PAD, gp.shape[1]), F32)
    gp[pl.ds(PAD + rows, PAD), :] = jnp.zeros((PAD, gp.shape[1]), F32)
    for i, copy in enumerate(local):
        if i not in (5, 6):
            copy.wait()
    pl.semaphore_wait(barrier, len(peers))

    dhalf = ffd // 2
    lanes = {
        VAL: (wab, (0, kz), None),
        GAT: (wab, (kz, kz), None),
        OUT: (wab, (2 * kz, 2 * kb), None),
        CP0: (wc, None, (0, 1)),
        CP1: (wc, None, (1, 1)),
        CP2: (wc, None, (2, EACH - 2)),
        CS: (wc, (0, kz // 2), (2 * EACH, 1)),
        CA: (wc, None, (2 * EACH + 1, 2)),
        CB: (wc, None, (2 * EACH + 3, 2)),
        DN: (wd, (0, dhalf), None),
    }
    ylane = {CP0: 0, CP1: 1, CP2: 2, CS: 3, DN: 4}

    def zslice(lane, idx, h=None, who=None):
        who = par if who is None else who
        ref, span, cols = lanes[lane]
        r0, n = (0, ref.shape[1]) if span is None else span
        if lane in (DN, CS):
            r0 = pl.multiple_of(who * n, 16)
        if h is not None:
            r0, n = r0 + h * (n // 2), n // 2
        if not isinstance(r0, int):
            r0 = pl.multiple_of(r0, 8)
        if cols is None:
            return ref.at[idx, pl.ds(r0, n)]
        c0 = cols[0] * LANE
        if lane in (CP0, CP1, CP2):
            c0 = pl.multiple_of(who * (EACH * LANE) + c0, LANE)
        return ref.at[idx, pl.ds(r0, n), pl.ds(c0, cols[1] * LANE)]

    def zidx(s, d):
        return lax.rem(fs - s + nf, nf) if d == 0 else lax.rem(fs + s, nf)

    near = half // 2

    def z_own(lane):
        for d in range(2):
            send(zslice(lane, fs), zs.at[lane], zr.at[lane, 0, d], zdev[d])

    def z_visit(lane, s):
        h = [None, None] if s < half else [0, 1]
        for d in range(2):
            idx = zidx(s, d)
            landed(zslice(lane, idx, h[d]), zr.at[lane, s - 1, d])
            if s < half:
                piece = zslice(lane, idx, d if s == half - 1 else None)
                send(piece, zs.at[lane], zr.at[lane, s, d], zdev[d])
        if lane in ylane:
            y, part = ylane[lane], 0 if s <= near else 1
            for d in range(2):
                send(zslice(lane, zidx(s, d), h[d]), ys.at[y], yr.at[y, part], peer_y)

    def y_done(lane, part):
        count = 2 * near if part == 0 else nf - 1 - 2 * near
        landed(zslice(lane, pl.ds(0, count), None, other), yr.at[ylane[lane], part])

    phases = ((VAL, GAT, OUT, CP0, CP1), (CP2, DN, CS, CA, CB))
    queue = [(lane, s) for group in phases for s in range(1, half + 1) for lane in group]

    def pump(n):
        for _ in range(min(n, len(queue))):
            lane, s = queue.pop(0)
            z_visit(lane, s)
            for now, later in zip(phases, phases[1:]):
                if s == half - 1 and lane == now[-1]:
                    for follow in later:
                        z_own(follow)

    def pump_to(lane, s):
        while (lane, s) in queue:
            pump(1)

    bufs = (tf, cf, mf)

    def blk(k, r, t, h=None):
        width = fc if k == CONV else fd
        r0, n = r * cr, cr
        if h is not None:
            r0, n = r0 + h * (cr // 2), cr // 2
        return bufs[k].at[pl.ds(r0, n), pl.ds(pl.multiple_of(t * width, width), width)]

    def ag_own(k, r):
        mine = blk(k, r, tp)
        send(mine, xs.at[k], xr.at[k, r, 0], right)
        send(mine, xs.at[k], xr.at[k, r, 1], left)
        send(mine, xs.at[k], xr.at[k, r, 4], partner)

    def ag_v1(k, r):
        for d, (src, onward) in enumerate(((tp_of(-1), right), (tp_of(1), left))):
            landed(blk(k, r, src), xr.at[k, r, d])
            send(blk(k, r, src, d), xs.at[k], xr.at[k, r, 2 + d], onward)
            send(blk(k, r, src), xs.at[k], xr.at[k, r, 4], partner)

    def ag_v2(k, r):
        for d in range(2):
            piece = blk(k, r, tp_of(2), d)
            landed(piece, xr.at[k, r, 2 + d])
            send(piece, xs.at[k], xr.at[k, r, 4], partner)

    def ag_done(k, r):
        width = fc if k == CONV else fd
        landed(bufs[k].at[pl.ds(r * cr, cr), pl.ds(0, nx * width)], xr.at[k, r, 4])

    tile = min(128, cr)

    def tiles(r, n, fn):
        def step(i, carry):
            fn(pl.multiple_of(r * cr + i * n, n))
            return carry

        lax.fori_loop(0, cr // n, step, 0)

    def norm(src, gain, r):
        def one(r0):
            total = jnp.zeros((tile, LANE), F32)
            for j in range(dm // LANE):
                v = src[pl.ds(r0, tile), pl.ds(j * LANE, LANE)].astype(F32)
                total = total + v * v
            scale = lax.rsqrt(jnp.sum(total, axis=-1, keepdims=True) / dm + 1e-06)
            for j in range(dm // LANE):
                cols = pl.ds(j * LANE, LANE)
                v = src[pl.ds(r0, tile), cols].astype(F32)
                nrm[pl.ds(r0, tile), cols] = (v * scale * gain[:, cols]).astype(BF16)

        tiles(r, tile, one)

    def mat_a(r):
        w = jnp.concatenate(
            [
                wab[:, 0:kz, :].reshape(dm, fc),
                wab[:, kz : 2 * kz, :].reshape(dm, fc),
            ],
            axis=1,
        )
        both = jnp.dot(nrm[pl.ds(r * cr, cr), :], w, preferred_element_type=F32)
        v, g = both[:, :fc], both[:, fc:]
        glu[pl.ds(PAD + r * cr, cr), :] = v / (1.0 + jnp.exp(-g))

    def conv(r):
        width = conv_taps.shape[0]
        base = PAD - (width - 1) // 2
        n = min(64, cr)

        def one(r0):
            total = jnp.zeros((n, fc), F32)
            for k in range(width):
                total = total + conv_taps[k : k + 1, :] * glu[pl.ds(r0 + base + k, n), :]
            cf[pl.ds(r0, n), pl.ds(pl.multiple_of(tp * fc, fc), fc)] = total.astype(BF16)

        tiles(r, n, one)

    def mix(r):
        def one(r0):
            s1 = jnp.zeros((tile, LANE), F32)
            s2 = jnp.zeros((tile, LANE), F32)
            for j in range(ca // LANE):
                v = cf[pl.ds(r0, tile), pl.ds(j * LANE, LANE)].astype(F32)
                s1 = s1 + v
                s2 = s2 + v * v
            mean = jnp.sum(s1, axis=-1, keepdims=True) / ca
            var = jnp.sum(s2, axis=-1, keepdims=True) / ca - mean * mean
            inv = lax.rsqrt(var + 1e-05)
            for j in range(ca // LANE):
                cols = pl.ds(j * LANE, LANE)
                v = cf[pl.ds(r0, tile), cols].astype(F32)
                v = (v - mean) * inv * chan_gain[:, cols] + chan_shift[:, cols]
                hm[pl.ds(r0, tile), cols] = (v / (1.0 + jnp.exp(-v))).astype(BF16)

        tiles(r, tile, one)
        w = jnp.concatenate(
            [
                wab[:, 2 * kz : 2 * kz + kb, :].reshape(ca, LANE),
                wab[:, 2 * kz + kb :, :].reshape(ca, LANE),
            ],
            axis=1,
        )
        here = pl.ds(r * cr, cr)
        prod = jnp.dot(hm[here, :], w, preferred_element_type=F32)
        mf[here, tok_cols] = (tf[here, tok_cols].astype(F32) + prod).astype(BF16)

    first_pairs = [(zidx(s, 0), zidx(s, 1)) for s in range(1, near + 1)]
    last_pairs = [(zidx(s, 0), zidx(s, 1)) for s in range(near + 1, half)] + [(fs, zidx(half, 0))]

    def pair_dots(r, pairs):
        here = pl.ds(r * cr, cr)
        total = None
        for pair in pairs:
            cols = [pl.ds(pl.multiple_of(i * kz, kz), kz) for i in pair]
            lhs = jnp.concatenate([nrm[here, c] for c in cols], axis=1)
            rhs = jnp.concatenate([wc[i] for i in pair], axis=0)
            term = jnp.dot(lhs, rhs, preferred_element_type=F32)
            total = term if total is None else total + term
        return total

    def mat_c(r):
        gp[pl.ds(PAD + r * cr, cr), :] = pair_dots(r, first_pairs)

    def mat_late(r):
        here = pl.ds(PAD + r * cr, cr)
        gp[here, :] = gp[here, :] + pair_dots(r, last_pairs)

    hr = rows // RCHUNKS
    hn = min(64, hr)

    def conv3(r0, at):
        cols = pl.ds(at * LANE, LANE)
        window = gp[pl.ds(pl.multiple_of(r0 + PAD - 8, 8), hn + 16), cols]
        total = c_taps[0:1, cols] * window[7 : 7 + hn]
        for k in range(1, gate_taps.shape[0]):
            total = total + c_taps[k : k + 1, cols] * window[7 + k : 7 + k + hn]
        return total

    def units(r0, j):
        g = conv3(r0, j if j < EACH else EACH + j)
        u = conv3(r0, EACH + j if j < EACH else whole + j)
        hh[pl.ds(r0, hn), pl.ds(j * LANE, LANE)] = (g / (1.0 + jnp.exp(-g)) * u).astype(BF16)

    def hidden(r):
        def step(i, carry):
            r0 = pl.multiple_of(r * hr + i * hn, hn)
            for j in range(whole):
                units(r0, j)
            v = conv3(r0, 2 * whole)
            u = pltpu.roll(v, LANE - tail, 1)
            h = (v / (1.0 + jnp.exp(-v)) * u).astype(BF16)
            hh[pl.ds(r0, hn), pl.ds(full_tiles, tail)] = h[:, :tail]
            return carry

        lax.fori_loop(0, hr // hn, step, 0)

    def down(r, m):
        w = jnp.concatenate([wd[2 * m], wd[2 * m + 1]], axis=1)
        return jnp.dot(hh[pl.ds(r * hr, hr), :], w, preferred_element_type=F32)

    hf = hr // 2

    def rs_a(r):
        for q in range(nx):
            qs[r, q] = down(r, 2 * q + 1 - co).astype(BF16)
        send(qs.at[r], rs.at[0], rr.at[r, 0], partner, qr.at[r])
        for q in range(nx):
            acc[r, q] = down(r, 2 * q + co)

    xr1, xl1, xo = lax.rem(xi + 1, nx), lax.rem(xi + nx - 1, nx), lax.rem(xi + 2, nx)

    def rs_b(r):
        landed(qr.at[r], rr.at[r, 0])
        far = acc[r, xo] + qr[r, xo].astype(F32)
        fs_[r] = far.astype(BF16)
        send(fs_.at[r, pl.ds(0, hf)], rs.at[1], rr.at[r, 1], right, fr.at[r, pl.ds(0, hf)])
        send(fs_.at[r, pl.ds(hf, hf)], rs.at[1], rr.at[r, 2], left, fr.at[r, pl.ds(hf, hf)])

    def rs_c(r):
        for d, (q, onward) in enumerate(((xr1, right), (xl1, left))):
            landed(fr.at[r, pl.ds(d * hf, hf)], rr.at[r, 1 + d])
            gets, keeps = pl.ds(d * hf, hf), pl.ds((1 - d) * hf, hf)
            both = acc[r, q, gets] + qr[r, q, gets].astype(F32) + fr[r, gets].astype(F32)
            ns[r, d, gets] = both.astype(BF16)
            ns[r, d, keeps] = (acc[r, q, keeps] + qr[r, q, keeps].astype(F32)).astype(BF16)
            send(ns.at[r, d], rs.at[2], rr.at[r, 3], onward, nr.at[r, d])

    def rs_d(r):
        here = pl.ds(r * hr, hr)
        total = acc[r, xi] + qr[r, xi].astype(F32) + mf[here, tok_cols].astype(F32)
        landed(nr.at[r], rr.at[r, 3])
        total = total + nr[r, 0].astype(F32) + nr[r, 1].astype(F32)
        sm[here, :] = total
        part = jnp.sum(total * total, axis=-1, keepdims=True)
        ss_send[r] = jnp.transpose(jnp.broadcast_to(part, (hr, LANE)))[0:8, :]
        for o in range(1, nt):
            send(
                ss_send.at[r],
                ts.at[0],
                tr.at[r],
                dev_tp(lax.rem(tp + o, nt)),
                ss_recv.at[r, o - 1],
            )

    def rs_e(r):
        here = pl.ds(r * hr, hr)
        total = ss_send[r]
        landed(ss_recv.at[r], tr.at[r])
        for o in range(nt - 1):
            total = total + ss_recv[r, o]
        wide = jnp.broadcast_to(total[0:1, :], (LANE, hr))
        scale = lax.rsqrt(jnp.transpose(wide)[:, 0:1] / dm + 1e-06)
        out[here, :] = (sm[here, :] * scale * final_gain[...]).astype(BF16)

    for lane in phases[0]:
        z_own(lane)
    ag_own(TOK, 0)
    ag_own(TOK, 1)
    for pos in range(2 * whole + 1):
        if pos not in soon:
            pack(pos)
    pump(5)
    ag_v1(TOK, 0)
    ag_own(TOK, 2)
    pump(5)
    ag_v1(TOK, 1)
    ag_own(TOK, 3)
    pump(5)
    ag_v2(TOK, 0)
    pump(3)
    ag_done(TOK, 0)
    norm(tf, mix_gain, 0)
    pump(2)
    ag_v1(TOK, 2)
    ag_v2(TOK, 1)
    pump(3)
    ag_done(TOK, 1)
    norm(tf, mix_gain, 1)
    pump(2)
    ag_v1(TOK, 3)
    pump(2)
    ag_v2(TOK, 2)
    pump(3)
    ag_done(TOK, 2)
    norm(tf, mix_gain, 2)
    ag_v2(TOK, 3)
    pump(3)
    ag_done(TOK, 3)
    norm(tf, mix_gain, 3)
    pump_to(GAT, half)
    mat_a(0)
    pump_to(CP1, half)
    for r in range(1, CHUNKS):
        mat_a(r)
        conv(r - 1)
        ag_own(CONV, r - 1)
        pump(1)
    conv(CHUNKS - 1)
    ag_own(CONV, CHUNKS - 1)
    pump(1)
    for r in range(CHUNKS):
        ag_v1(CONV, r)
        pump(1)
    ag_v2(CONV, 0)
    ag_v2(CONV, 1)
    pump(1)
    for r in range(CHUNKS):
        ag_done(CONV, r)
        mix(r)
        ag_own(MIX, r)
        pump(1)
        if r + 2 < CHUNKS:
            ag_v2(CONV, r + 2)
    for r in range(CHUNKS):
        pump(2 if r != CHUNKS - 1 else 3)
        ag_v1(MIX, r)
    for r in range(CHUNKS):
        ag_v2(MIX, r)
        pump(2 if r < 2 else 1)
    for r in range(CHUNKS):
        ag_done(MIX, r)
        norm(mf, mlp_gain, r)
        pump(1)
    pump_to(CB, near)
    for lane in (CP0, CP1, CP2, CS):
        y_done(lane, 0)
    for r in range(CHUNKS):
        mat_c(r)
        pump(1)
    pump(len(queue))
    for lane in (CP0, CP1, CP2, CS):
        y_done(lane, 1)
    per = cr // hr

    def if_chunk(stage, r):
        if 0 <= r < RCHUNKS:
            stage(r)

    for tick in range(RCHUNKS + 10):
        late = False
        if tick < RCHUNKS:
            if tick == 0:
                mat_late(0)
            if tick % per == per - 1 and tick // per + 1 < CHUNKS:
                mat_late(tick // per + 1)
                late = True
            hidden(tick)
            if tick == 0:
                y_done(DN, 0)
                y_done(DN, 1)
        if_chunk(rs_c, tick - 3)
        if late or tick >= RCHUNKS:
            if_chunk(rs_b, tick - 1)
        if tick < RCHUNKS:
            rs_a(tick)
            if not late:
                if_chunk(rs_b, tick - 1)
        if_chunk(rs_d, tick - 7)
        if_chunk(rs_e, tick - 10)

    for lane in lanes:
        left_here(zslice(lane, pl.ds(0, nf - 1)), zs.at[lane])
        if lane in ylane:
            left_here(zslice(lane, pl.ds(0, nf - 1)), ys.at[ylane[lane]])
    for k, width in ((TOK, fd), (CONV, fc), (MIX, fd)):
        left_here(bufs[k].at[:, pl.ds(0, (nt - 1) * width)], xs.at[k])
    for i, ref in enumerate((qs, fs_, ns)):
        left_here(ref, rs.at[i])
    left_here(ss_recv, ts.at[0])


def local(mesh, *args):
    (
        tokens,
        mix_gain,
        value_proj,
        gate_proj,
        conv_taps,
        chan_gain,
        chan_shift,
        mix_out,
        mlp_gain,
        mlp_gate,
        mlp_up,
        gate_taps,
        up_taps,
        mlp_down,
        final_gain,
    ) = args
    nf, nt = mesh.shape["fs"], mesh.shape["tp"]
    nx = nt // 2
    rows, fd = tokens.shape
    dm = mix_gain.shape[0]
    ca = chan_gain.shape[0]
    fc = value_proj.shape[1]
    kz, ffd = mlp_gate.shape
    kb = mix_out.shape[0]
    hr = rows // RCHUNKS
    half = nf // 2
    row = lambda v: v.reshape(1, -1)
    hbm = pl.BlockSpec(memory_space=pltpu.HBM)
    vmem = pl.BlockSpec(memory_space=pltpu.VMEM)
    dma = pltpu.SemaphoreType.DMA
    return pl.pallas_call(
        functools.partial(body, (nf, nt)),
        out_shape=jax.ShapeDtypeStruct((rows, fd), BF16),
        in_specs=[hbm, vmem, hbm, hbm, vmem, vmem, vmem, hbm, vmem, hbm, hbm, vmem, vmem, hbm, vmem],
        out_specs=vmem,
        scratch_shapes=[
            pltpu.VMEM((nf, 2 * kz + 2 * kb, LANE), BF16),
            pltpu.VMEM((nf, kz, 2 * ffd), BF16),
            pltpu.VMEM((nf, ffd, mlp_down.shape[1]), BF16),
            pltpu.VMEM((rows, dm), BF16),
            pltpu.VMEM((rows, ca), BF16),
            pltpu.VMEM((rows, dm), BF16),
            pltpu.VMEM((rows, dm), BF16),
            pltpu.VMEM((rows + 2 * PAD, fc), F32),
            pltpu.VMEM((rows + 2 * PAD, 2 * ffd), F32),
            pltpu.VMEM((rows, ca), BF16),
            pltpu.VMEM((rows, ffd), BF16),
            pltpu.VMEM((RCHUNKS, nx, hr, fd), F32),
            pltpu.VMEM((RCHUNKS, nx, hr, fd), BF16),
            pltpu.VMEM((RCHUNKS, nx, hr, fd), BF16),
            pltpu.VMEM((RCHUNKS, hr, fd), BF16),
            pltpu.VMEM((RCHUNKS, hr, fd), BF16),
            pltpu.VMEM((RCHUNKS, 2, hr, fd), BF16),
            pltpu.VMEM((RCHUNKS, 2, hr, fd), BF16),
            pltpu.VMEM((rows, fd), F32),
            pltpu.VMEM((RCHUNKS, 8, hr), F32),
            pltpu.VMEM((RCHUNKS, nt - 1, 8, hr), F32),
            pltpu.VMEM((ffd, kz), BF16),
            pltpu.VMEM((ffd, kz), BF16),
            pltpu.VMEM((8, 2 * ffd), F32),
            dma((8,)),
            dma((10,)),
            dma((10, half, 2)),
            dma((5,)),
            dma((5, 2)),
            dma((3,)),
            dma((3, CHUNKS, 5)),
            dma((3,)),
            dma((RCHUNKS, 4)),
            dma((1,)),
            dma((RCHUNKS,)),
        ],
        compiler_params=pltpu.CompilerParams(
            collective_id=0, has_side_effects=True, vmem_limit_bytes=67043328
        ),
        name="layer",
    )(
        tokens,
        row(mix_gain),
        value_proj,
        gate_proj,
        conv_taps,
        row(chan_gain),
        row(chan_shift),
        mix_out,
        row(mlp_gain),
        mlp_gate.T,
        mlp_up.T,
        gate_taps,
        up_taps,
        mlp_down,
        row(final_gain),
    )


def solution(mesh):
    return jax.shard_map(
        functools.partial(local, mesh),
        mesh=mesh,
        in_specs=(
            P(("grp", "fs"), "tp"),
            P(),
            P("fs", "tp"),
            P("fs", "tp"),
            P(None, "tp"),
            P(),
            P(),
            P("fs", "tp"),
            P(),
            P("fs", "tp"),
            P("fs", "tp"),
            P(None, "tp"),
            P(None, "tp"),
            P("tp", "fs"),
            P("tp"),
        ),
        out_specs=P(("grp", "fs"), "tp"),
        check_vma=False,
    )
```

```python
import functools

import jax
import jax.numpy as jnp
from jax import lax
from jax.experimental import pallas as pl
from jax.experimental.pallas import tpu as pltpu
from jax.sharding import PartitionSpec as P

F32 = jnp.float32
BF16 = jnp.bfloat16
CHUNKS = 4
RCHUNKS = 8
LANE = 128
PAD = 16
EACH = 3
VAL, GAT, OUT, CP0, CP1, CP2, CS, CA, CB, DN = range(10)
TOK, CONV, MIX = range(3)


def body(
    sizes,
    tokens,
    mix_gain,
    value_own,
    gate_own,
    conv_taps,
    chan_gain,
    chan_shift,
    mix_out_own,
    mlp_gain,
    mlp_gate,
    mlp_up,
    gate_taps,
    up_taps,
    d_own,
    final_gain,
    out,
    wab,
    wc,
    wd,
    tf,
    cf,
    mf,
    nrm,
    glu,
    gp,
    hm,
    hh,
    acc,
    qs,
    qr,
    fs_,
    fr,
    ns,
    nr,
    sm,
    ss_send,
    ss_recv,
    gbuf,
    ubuf,
    c_taps,
    lsem,
    zs,
    zr,
    ys,
    yr,
    xs,
    xr,
    rs,
    rr,
    ts,
    tr,
):
    nf, nt = sizes
    nx = nt // 2
    half = nf // 2
    rows, fd = tokens.shape
    dm = tf.shape[1]
    ca = cf.shape[1]
    fc = ca // nt
    cr = rows // CHUNKS
    ffd = hh.shape[1]
    full_tiles = ffd // LANE * LANE
    tail = ffd - full_tiles
    kz = value_own.shape[0]
    kb = mix_out_own.shape[0]

    grp = lax.axis_index("grp")
    fs = lax.axis_index("fs")
    tp = lax.axis_index("tp")
    xi = tp // 2
    co = lax.rem(tp, 2)
    par = lax.rem(grp, 2)
    other = 1 - par

    def tp_of(dx, flip=False):
        core = 1 - co if flip else co
        return lax.rem(xi + dx + nx, nx) * 2 + core

    def dev_tp(t):
        return (grp, fs, t)

    def dev_fs(d):
        return (grp, lax.rem(fs + d + nf, nf), tp)

    peer_y = (grp + 1 - 2 * par, fs, tp)
    right, left, partner = dev_tp(tp_of(1)), dev_tp(tp_of(-1)), dev_tp(tp_of(0, True))
    zdev = (dev_fs(1), dev_fs(-1))

    def remote(src, dst, ssem, rsem, dev):
        return pltpu.make_async_remote_copy(
            src_ref=src,
            dst_ref=dst,
            send_sem=ssem,
            recv_sem=rsem,
            device_id=dev,
            device_id_type=pl.DeviceIdType.MESH,
        )

    def send(ref, ssem, rsem, dev, dst=None):
        remote(ref, ref if dst is None else dst, ssem, rsem, dev).start()

    def landed(ref, sem):
        remote(ref, ref, sem, sem, partner).wait_recv()

    def left_here(ref, sem):
        remote(ref, ref, sem, sem, partner).wait_send()

    barrier = pltpu.get_barrier_semaphore()
    peers = [dev_tp(lax.rem(tp + o, nt)) for o in range(1, nt)] + [zdev[0], zdev[1], peer_y]
    for dev in peers:
        pl.semaphore_signal(barrier, inc=1, device_id=dev, device_id_type=pl.DeviceIdType.MESH)

    def own_c(r0, n):
        return wc.at[fs, pl.ds(r0, n)]

    tok_cols = pl.ds(pl.multiple_of(tp * fd, fd), fd)
    moves = [
        (value_own, wab.at[fs, pl.ds(0, kz)]),
        (gate_own, wab.at[fs, pl.ds(kz, kz)]),
        (mix_out_own.at[:, pl.ds(0, LANE)], wab.at[fs, pl.ds(2 * kz, kb)]),
        (mix_out_own.at[:, pl.ds(LANE, LANE)], wab.at[fs, pl.ds(2 * kz + kb, kb)]),
        (tokens, tf.at[:, tok_cols]),
        (mlp_gate, gbuf),
        (mlp_up, ubuf),
        (d_own, wd.at[fs]),
    ]
    local = [pltpu.make_async_copy(a, b, lsem.at[i]) for i, (a, b) in enumerate(moves)]
    for copy in local:
        copy.start()

    whole = full_tiles // LANE
    cut = EACH * LANE
    at = 0
    for taps, lo, hi in (
        (gate_taps, 0, cut),
        (up_taps, 0, cut),
        (gate_taps, cut, full_tiles),
        (up_taps, cut, full_tiles),
        (gate_taps, full_tiles, ffd),
        (up_taps, full_tiles, ffd),
    ):
        c_taps[0 : taps.shape[0], at : at + hi - lo] = taps[:, lo:hi]
        at += hi - lo

    def pack(pos):
        if pos == 2 * whole:
            piece = jnp.concatenate([gbuf[full_tiles:, :], ubuf[full_tiles:, :]], axis=0)
        else:
            if pos < 2 * EACH:
                src, j = (gbuf, pos) if pos < EACH else (ubuf, pos - EACH)
            else:
                src, j = (gbuf, pos - EACH) if pos < EACH + whole else (ubuf, pos - whole)
            piece = src[j * LANE : (j + 1) * LANE, :]
        turned = jnp.transpose(piece.astype(F32)).astype(BF16)
        wc[fs, :, pos * LANE : (pos + 1) * LANE] = turned

    for i in (5, 6):
        local[i].wait()
    soon = (0, 1, EACH, EACH + 1)
    for pos in soon:
        pack(pos)

    glu[pl.ds(0, PAD), :] = jnp.zeros((PAD, fc), F32)
    glu[pl.ds(PAD + rows, PAD), :] = jnp.zeros((PAD, fc), F32)
    gp[pl.ds(0, PAD), :] = jnp.zeros((PAD, gp.shape[1]), F32)
    gp[pl.ds(PAD + rows, PAD), :] = jnp.zeros((PAD, gp.shape[1]), F32)
    for i, copy in enumerate(local):
        if i not in (5, 6):
            copy.wait()
    pl.semaphore_wait(barrier, len(peers))

    dhalf = ffd // 2
    lanes = {
        VAL: (wab, (0, kz), None),
        GAT: (wab, (kz, kz), None),
        OUT: (wab, (2 * kz, 2 * kb), None),
        CP0: (wc, None, (0, 1)),
        CP1: (wc, None, (1, 1)),
        CP2: (wc, None, (2, EACH - 2)),
        CS: (wc, (0, kz // 2), (2 * EACH, 1)),
        CA: (wc, None, (2 * EACH + 1, 2)),
        CB: (wc, None, (2 * EACH + 3, 2)),
        DN: (wd, (0, dhalf), None),
    }
    ylane = {CP0: 0, CP1: 1, CP2: 2, CS: 3, DN: 4}

    def zslice(lane, idx, h=None, who=None):
        who = par if who is None else who
        ref, span, cols = lanes[lane]
        r0, n = (0, ref.shape[1]) if span is None else span
        if lane in (DN, CS):
            r0 = pl.multiple_of(who * n, 16)
        if h is not None:
            r0, n = r0 + h * (n // 2), n // 2
        if not isinstance(r0, int):
            r0 = pl.multiple_of(r0, 8)
        if cols is None:
            return ref.at[idx, pl.ds(r0, n)]
        c0 = cols[0] * LANE
        if lane in (CP0, CP1, CP2):
            c0 = pl.multiple_of(who * (EACH * LANE) + c0, LANE)
        return ref.at[idx, pl.ds(r0, n), pl.ds(c0, cols[1] * LANE)]

    def zidx(s, d):
        return lax.rem(fs - s + nf, nf) if d == 0 else lax.rem(fs + s, nf)

    near = half // 2

    def z_own(lane):
        for d in range(2):
            send(zslice(lane, fs), zs.at[lane], zr.at[lane, 0, d], zdev[d])

    def z_visit(lane, s):
        h = [None, None] if s < half else [0, 1]
        for d in range(2):
            idx = zidx(s, d)
            landed(zslice(lane, idx, h[d]), zr.at[lane, s - 1, d])
            if s < half:
                piece = zslice(lane, idx, d if s == half - 1 else None)
                send(piece, zs.at[lane], zr.at[lane, s, d], zdev[d])
        if lane in ylane:
            y, part = ylane[lane], 0 if s <= near else 1
            for d in range(2):
                send(zslice(lane, zidx(s, d), h[d]), ys.at[y], yr.at[y, part], peer_y)

    def y_done(lane, part):
        count = 2 * near if part == 0 else nf - 1 - 2 * near
        landed(zslice(lane, pl.ds(0, count), None, other), yr.at[ylane[lane], part])

    phases = ((VAL, GAT, OUT, CP0, CP1), (CP2, CS, DN, CA, CB))
    queue = [(lane, s) for group in phases for s in range(1, half + 1) for lane in group]

    def pump(n):
        for _ in range(min(n, len(queue))):
            lane, s = queue.pop(0)
            z_visit(lane, s)
            for now, later in zip(phases, phases[1:]):
                if s == half - 1 and lane == now[-1]:
                    for follow in later:
                        z_own(follow)

    def pump_to(lane, s):
        while (lane, s) in queue:
            pump(1)

    bufs = (tf, cf, mf)

    def blk(k, r, t, h=None):
        width = fc if k == CONV else fd
        r0, n = r * cr, cr
        if h is not None:
            r0, n = r0 + h * (cr // 2), cr // 2
        return bufs[k].at[pl.ds(r0, n), pl.ds(pl.multiple_of(t * width, width), width)]

    def ag_own(k, r):
        mine = blk(k, r, tp)
        send(mine, xs.at[k], xr.at[k, r, 0], right)
        send(mine, xs.at[k], xr.at[k, r, 1], left)
        send(mine, xs.at[k], xr.at[k, r, 4], partner)

    def ag_v1(k, r):
        for d, (src, onward) in enumerate(((tp_of(-1), right), (tp_of(1), left))):
            landed(blk(k, r, src), xr.at[k, r, d])
            send(blk(k, r, src, d), xs.at[k], xr.at[k, r, 2 + d], onward)
            send(blk(k, r, src), xs.at[k], xr.at[k, r, 4], partner)

    def ag_v2(k, r):
        for d in range(2):
            piece = blk(k, r, tp_of(2), d)
            landed(piece, xr.at[k, r, 2 + d])
            send(piece, xs.at[k], xr.at[k, r, 4], partner)

    def ag_done(k, r):
        width = fc if k == CONV else fd
        landed(bufs[k].at[pl.ds(r * cr, cr), pl.ds(0, nx * width)], xr.at[k, r, 4])

    tile = min(128, cr)

    def tiles(r, n, fn):
        def step(i, carry):
            fn(pl.multiple_of(r * cr + i * n, n))
            return carry

        lax.fori_loop(0, cr // n, step, 0)

    def norm(src, gain, r):
        def one(r0):
            total = jnp.zeros((tile, LANE), F32)
            for j in range(dm // LANE):
                v = src[pl.ds(r0, tile), pl.ds(j * LANE, LANE)].astype(F32)
                total = total + v * v
            scale = lax.rsqrt(jnp.sum(total, axis=-1, keepdims=True) / dm + 1e-06)
            for j in range(dm // LANE):
                cols = pl.ds(j * LANE, LANE)
                v = src[pl.ds(r0, tile), cols].astype(F32)
                nrm[pl.ds(r0, tile), cols] = (v * scale * gain[:, cols]).astype(BF16)

        tiles(r, tile, one)

    def mat_a(r):
        w = jnp.concatenate(
            [
                wab[:, 0:kz, :].reshape(dm, fc),
                wab[:, kz : 2 * kz, :].reshape(dm, fc),
            ],
            axis=1,
        )
        both = jnp.dot(nrm[pl.ds(r * cr, cr), :], w, preferred_element_type=F32)
        v, g = both[:, :fc], both[:, fc:]
        glu[pl.ds(PAD + r * cr, cr), :] = v / (1.0 + jnp.exp(-g))

    def conv(r):
        width = conv_taps.shape[0]
        base = PAD - (width - 1) // 2
        n = min(64, cr)

        def one(r0):
            total = jnp.zeros((n, fc), F32)
            for k in range(width):
                total = total + conv_taps[k : k + 1, :] * glu[pl.ds(r0 + base + k, n), :]
            cf[pl.ds(r0, n), pl.ds(pl.multiple_of(tp * fc, fc), fc)] = total.astype(BF16)

        tiles(r, n, one)

    def mix(r):
        def one(r0):
            s1 = jnp.zeros((tile, LANE), F32)
            s2 = jnp.zeros((tile, LANE), F32)
            for j in range(ca // LANE):
                v = cf[pl.ds(r0, tile), pl.ds(j * LANE, LANE)].astype(F32)
                s1 = s1 + v
                s2 = s2 + v * v
            mean = jnp.sum(s1, axis=-1, keepdims=True) / ca
            var = jnp.sum(s2, axis=-1, keepdims=True) / ca - mean * mean
            inv = lax.rsqrt(var + 1e-05)
            for j in range(ca // LANE):
                cols = pl.ds(j * LANE, LANE)
                v = cf[pl.ds(r0, tile), cols].astype(F32)
                v = (v - mean) * inv * chan_gain[:, cols] + chan_shift[:, cols]
                hm[pl.ds(r0, tile), cols] = (v / (1.0 + jnp.exp(-v))).astype(BF16)

        tiles(r, tile, one)
        w = jnp.concatenate(
            [
                wab[:, 2 * kz : 2 * kz + kb, :].reshape(ca, LANE),
                wab[:, 2 * kz + kb :, :].reshape(ca, LANE),
            ],
            axis=1,
        )
        here = pl.ds(r * cr, cr)
        prod = jnp.dot(hm[here, :], w, preferred_element_type=F32)
        mf[here, tok_cols] = (tf[here, tok_cols].astype(F32) + prod).astype(BF16)

    first_pairs = [(zidx(s, 0), zidx(s, 1)) for s in range(1, near + 1)]
    last_pairs = [(zidx(s, 0), zidx(s, 1)) for s in range(near + 1, half)] + [(fs, zidx(half, 0))]

    def pair_dots(r, pairs):
        here = pl.ds(r * cr, cr)
        total = None
        for pair in pairs:
            cols = [pl.ds(pl.multiple_of(i * kz, kz), kz) for i in pair]
            lhs = jnp.concatenate([nrm[here, c] for c in cols], axis=1)
            rhs = jnp.concatenate([wc[i] for i in pair], axis=0)
            term = jnp.dot(lhs, rhs, preferred_element_type=F32)
            total = term if total is None else total + term
        return total

    def mat_c(r):
        gp[pl.ds(PAD + r * cr, cr), :] = pair_dots(r, first_pairs)

    def mat_late(r):
        here = pl.ds(PAD + r * cr, cr)
        gp[here, :] = gp[here, :] + pair_dots(r, last_pairs)

    hr = rows // RCHUNKS
    hn = min(64, hr)

    def conv3(r0, at):
        cols = pl.ds(at * LANE, LANE)
        window = gp[pl.ds(pl.multiple_of(r0 + PAD - 8, 8), hn + 16), cols]
        total = c_taps[0:1, cols] * window[7 : 7 + hn]
        for k in range(1, gate_taps.shape[0]):
            total = total + c_taps[k : k + 1, cols] * window[7 + k : 7 + k + hn]
        return total

    def units(r0, j):
        g = conv3(r0, j if j < EACH else EACH + j)
        u = conv3(r0, EACH + j if j < EACH else whole + j)
        hh[pl.ds(r0, hn), pl.ds(j * LANE, LANE)] = (g / (1.0 + jnp.exp(-g)) * u).astype(BF16)

    def hidden(r):
        def step(i, carry):
            r0 = pl.multiple_of(r * hr + i * hn, hn)
            for j in range(whole):
                units(r0, j)
            v = conv3(r0, 2 * whole)
            u = pltpu.roll(v, LANE - tail, 1)
            h = (v / (1.0 + jnp.exp(-v)) * u).astype(BF16)
            hh[pl.ds(r0, hn), pl.ds(full_tiles, tail)] = h[:, :tail]
            return carry

        lax.fori_loop(0, hr // hn, step, 0)

    def down(r, m):
        w = jnp.concatenate([wd[2 * m], wd[2 * m + 1]], axis=1)
        return jnp.dot(hh[pl.ds(r * hr, hr), :], w, preferred_element_type=F32)

    hf = hr // 2

    def rs_a(r):
        for q in range(nx):
            qs[r, q] = down(r, 2 * q + 1 - co).astype(BF16)
        send(qs.at[r], rs.at[0], rr.at[r, 0], partner, qr.at[r])
        for q in range(nx):
            acc[r, q] = down(r, 2 * q + co)

    xr1, xl1, xo = lax.rem(xi + 1, nx), lax.rem(xi + nx - 1, nx), lax.rem(xi + 2, nx)

    def rs_b(r):
        landed(qr.at[r], rr.at[r, 0])
        far = acc[r, xo] + qr[r, xo].astype(F32)
        fs_[r] = far.astype(BF16)
        send(fs_.at[r, pl.ds(0, hf)], rs.at[1], rr.at[r, 1], right, fr.at[r, pl.ds(0, hf)])
        send(fs_.at[r, pl.ds(hf, hf)], rs.at[1], rr.at[r, 2], left, fr.at[r, pl.ds(hf, hf)])

    def rs_c(r):
        for d, (q, onward) in enumerate(((xr1, right), (xl1, left))):
            landed(fr.at[r, pl.ds(d * hf, hf)], rr.at[r, 1 + d])
            gets, keeps = pl.ds(d * hf, hf), pl.ds((1 - d) * hf, hf)
            both = acc[r, q, gets] + qr[r, q, gets].astype(F32) + fr[r, gets].astype(F32)
            ns[r, d, gets] = both.astype(BF16)
            ns[r, d, keeps] = (acc[r, q, keeps] + qr[r, q, keeps].astype(F32)).astype(BF16)
            send(ns.at[r, d], rs.at[2], rr.at[r, 3], onward, nr.at[r, d])

    def rs_d(r):
        here = pl.ds(r * hr, hr)
        total = acc[r, xi] + qr[r, xi].astype(F32) + mf[here, tok_cols].astype(F32)
        landed(nr.at[r], rr.at[r, 3])
        total = total + nr[r, 0].astype(F32) + nr[r, 1].astype(F32)
        sm[here, :] = total
        part = jnp.sum(total * total, axis=-1, keepdims=True)
        ss_send[r] = jnp.transpose(jnp.broadcast_to(part, (hr, LANE)))[0:8, :]
        for o in range(1, nt):
            send(
                ss_send.at[r],
                ts.at[0],
                tr.at[r],
                dev_tp(lax.rem(tp + o, nt)),
                ss_recv.at[r, o - 1],
            )

    def rs_e(r):
        here = pl.ds(r * hr, hr)
        total = ss_send[r]
        landed(ss_recv.at[r], tr.at[r])
        for o in range(nt - 1):
            total = total + ss_recv[r, o]
        wide = jnp.broadcast_to(total[0:1, :], (LANE, hr))
        scale = lax.rsqrt(jnp.transpose(wide)[:, 0:1] / dm + 1e-06)
        out[here, :] = (sm[here, :] * scale * final_gain[...]).astype(BF16)

    for lane in phases[0]:
        z_own(lane)
    ag_own(TOK, 0)
    ag_own(TOK, 1)
    for pos in range(2 * whole + 1):
        if pos not in soon:
            pack(pos)
    pump(5)
    ag_v1(TOK, 0)
    ag_own(TOK, 2)
    pump(5)
    ag_v1(TOK, 1)
    ag_own(TOK, 3)
    pump(5)
    ag_v2(TOK, 0)
    pump(3)
    ag_done(TOK, 0)
    norm(tf, mix_gain, 0)
    pump(2)
    ag_v1(TOK, 2)
    ag_v2(TOK, 1)
    pump(3)
    ag_done(TOK, 1)
    norm(tf, mix_gain, 1)
    pump(2)
    ag_v1(TOK, 3)
    pump(2)
    ag_v2(TOK, 2)
    pump(3)
    ag_done(TOK, 2)
    norm(tf, mix_gain, 2)
    ag_v2(TOK, 3)
    pump(3)
    ag_done(TOK, 3)
    norm(tf, mix_gain, 3)
    pump_to(GAT, half)
    mat_a(0)
    pump_to(CP1, half)
    for r in range(1, CHUNKS):
        mat_a(r)
        conv(r - 1)
        ag_own(CONV, r - 1)
        pump(1)
    conv(CHUNKS - 1)
    ag_own(CONV, CHUNKS - 1)
    pump(1)
    for r in range(CHUNKS):
        ag_v1(CONV, r)
        pump(1)
    ag_v2(CONV, 0)
    ag_v2(CONV, 1)
    pump(1)
    for r in range(CHUNKS):
        ag_done(CONV, r)
        mix(r)
        ag_own(MIX, r)
        pump(1)
        if r + 2 < CHUNKS:
            ag_v2(CONV, r + 2)
    for r in range(CHUNKS):
        pump(2 if r != CHUNKS - 1 else 3)
        ag_v1(MIX, r)
    for r in range(CHUNKS):
        ag_v2(MIX, r)
        pump(2 if r < 2 else 1)
    for r in range(CHUNKS):
        ag_done(MIX, r)
        norm(mf, mlp_gain, r)
        pump(1)
    pump_to(CB, near)
    for lane in (CP0, CP1, CP2, CS):
        y_done(lane, 0)
    for r in range(CHUNKS):
        mat_c(r)
        pump(1)
    pump(len(queue))
    for lane in (CP0, CP1, CP2, CS):
        y_done(lane, 1)
    per = cr // hr

    def if_chunk(stage, r):
        if 0 <= r < RCHUNKS:
            stage(r)

    for tick in range(RCHUNKS + 10):
        late = False
        if tick < RCHUNKS:
            if tick == 0:
                mat_late(0)
            if tick % per == per - 1 and tick // per + 1 < CHUNKS:
                mat_late(tick // per + 1)
                late = True
            hidden(tick)
            if tick == 0:
                y_done(DN, 0)
                y_done(DN, 1)
        if late or tick >= RCHUNKS:
            if_chunk(rs_b, tick - 1)
        if tick < RCHUNKS:
            rs_a(tick)
            if not late:
                if_chunk(rs_b, tick - 1)
        if_chunk(rs_c, tick - 3)
        if_chunk(rs_d, tick - 7)
        if_chunk(rs_e, tick - 10)

    for lane in lanes:
        left_here(zslice(lane, pl.ds(0, nf - 1)), zs.at[lane])
        if lane in ylane:
            left_here(zslice(lane, pl.ds(0, nf - 1)), ys.at[ylane[lane]])
    for k, width in ((TOK, fd), (CONV, fc), (MIX, fd)):
        left_here(bufs[k].at[:, pl.ds(0, (nt - 1) * width)], xs.at[k])
    for i, ref in enumerate((qs, fs_, ns)):
        left_here(ref, rs.at[i])
    left_here(ss_recv, ts.at[0])


def local(mesh, *args):
    (
        tokens,
        mix_gain,
        value_proj,
        gate_proj,
        conv_taps,
        chan_gain,
        chan_shift,
        mix_out,
        mlp_gain,
        mlp_gate,
        mlp_up,
        gate_taps,
        up_taps,
        mlp_down,
        final_gain,
    ) = args
    nf, nt = mesh.shape["fs"], mesh.shape["tp"]
    nx = nt // 2
    rows, fd = tokens.shape
    dm = mix_gain.shape[0]
    ca = chan_gain.shape[0]
    fc = value_proj.shape[1]
    kz, ffd = mlp_gate.shape
    kb = mix_out.shape[0]
    hr = rows // RCHUNKS
    half = nf // 2
    row = lambda v: v.reshape(1, -1)
    hbm = pl.BlockSpec(memory_space=pltpu.HBM)
    vmem = pl.BlockSpec(memory_space=pltpu.VMEM)
    dma = pltpu.SemaphoreType.DMA
    return pl.pallas_call(
        functools.partial(body, (nf, nt)),
        out_shape=jax.ShapeDtypeStruct((rows, fd), BF16),
        in_specs=[hbm, vmem, hbm, hbm, vmem, vmem, vmem, hbm, vmem, hbm, hbm, vmem, vmem, hbm, vmem],
        out_specs=vmem,
        scratch_shapes=[
            pltpu.VMEM((nf, 2 * kz + 2 * kb, LANE), BF16),
            pltpu.VMEM((nf, kz, 2 * ffd), BF16),
            pltpu.VMEM((nf, ffd, mlp_down.shape[1]), BF16),
            pltpu.VMEM((rows, dm), BF16),
            pltpu.VMEM((rows, ca), BF16),
            pltpu.VMEM((rows, dm), BF16),
            pltpu.VMEM((rows, dm), BF16),
            pltpu.VMEM((rows + 2 * PAD, fc), F32),
            pltpu.VMEM((rows + 2 * PAD, 2 * ffd), F32),
            pltpu.VMEM((rows, ca), BF16),
            pltpu.VMEM((rows, ffd), BF16),
            pltpu.VMEM((RCHUNKS, nx, hr, fd), F32),
            pltpu.VMEM((RCHUNKS, nx, hr, fd), BF16),
            pltpu.VMEM((RCHUNKS, nx, hr, fd), BF16),
            pltpu.VMEM((RCHUNKS, hr, fd), BF16),
            pltpu.VMEM((RCHUNKS, hr, fd), BF16),
            pltpu.VMEM((RCHUNKS, 2, hr, fd), BF16),
            pltpu.VMEM((RCHUNKS, 2, hr, fd), BF16),
            pltpu.VMEM((rows, fd), F32),
            pltpu.VMEM((RCHUNKS, 8, hr), F32),
            pltpu.VMEM((RCHUNKS, nt - 1, 8, hr), F32),
            pltpu.VMEM((ffd, kz), BF16),
            pltpu.VMEM((ffd, kz), BF16),
            pltpu.VMEM((8, 2 * ffd), F32),
            dma((8,)),
            dma((10,)),
            dma((10, half, 2)),
            dma((5,)),
            dma((5, 2)),
            dma((3,)),
            dma((3, CHUNKS, 5)),
            dma((3,)),
            dma((RCHUNKS, 4)),
            dma((1,)),
            dma((RCHUNKS,)),
        ],
        compiler_params=pltpu.CompilerParams(
            collective_id=0, has_side_effects=True, vmem_limit_bytes=67043328
        ),
        name="layer",
    )(
        tokens,
        row(mix_gain),
        value_proj,
        gate_proj,
        conv_taps,
        row(chan_gain),
        row(chan_shift),
        mix_out,
        row(mlp_gain),
        mlp_gate.T,
        mlp_up.T,
        gate_taps,
        up_taps,
        mlp_down,
        row(final_gain),
    )


def solution(mesh):
    return jax.shard_map(
        functools.partial(local, mesh),
        mesh=mesh,
        in_specs=(
            P(("grp", "fs"), "tp"),
            P(),
            P("fs", "tp"),
            P("fs", "tp"),
            P(None, "tp"),
            P(),
            P(),
            P("fs", "tp"),
            P(),
            P("fs", "tp"),
            P("fs", "tp"),
            P(None, "tp"),
            P(None, "tp"),
            P("tp", "fs"),
            P("tp"),
        ),
        out_specs=P(("grp", "fs"), "tp"),
        check_vma=False,
    )
```
